512 devices in a mesh: sp: 64 (over z, y), fs: 4 (over x), tp: 2 (over core).
Axes of the slice: x: 4, y: 8, z: 8, core: 2. Of those that a mesh axis runs over, the one named last changes fastest.
Arguments:
- tokens: bfloat16 [4, 16384, 1024], P('fs', 'sp', 'tp'), may hold values from -6 to 6
- w_inner: bfloat16 [1024, 2048], P('sp', 'tp'), may hold values from -0.1875 to 0.1875
- w_gate: bfloat16 [1024, 2048], P('sp', 'tp'), may hold values from -0.1875 to 0.1875
- w_write: bfloat16 [1024, 512], P('sp', 'tp'), may hold values from -0.1875 to 0.1875
- w_read: bfloat16 [1024, 512], P('sp', 'tp'), may hold values from -0.1875 to 0.1875
- w_pool_in: bfloat16 [1024, 1024], P('sp', 'tp'), may hold values from -0.1875 to 0.1875
- w_step: bfloat16 [1024, 2, 32], replicated, may hold values from -0.1875 to 0.1875
- conv_inner: bfloat16 [5, 2048], replicated, may hold values from -2.5 to 2.5
- conv_cross: bfloat16 [5, 2, 512], replicated, may hold values from -2.5 to 2.5
- rate_log: float32 [2, 32], replicated, may hold values from -20 to -3
- decay_extra: float32 [4, 16384, 2, 32], P('fs', 'sp', None, 'tp'), may hold values from -1 to 0
- norm_gain: float32 [2048], replicated, may hold values from 0.1 to 1.9
- pool_mix: bfloat16 [4, 256, 256], replicated, may hold values from -0.375 to 0.375
- pool_gain: float32 [1024], replicated, may hold values from 0.1 to 1.9
- w_out_inner: bfloat16 [2048, 1024], P('tp', 'fs'), may hold values from -0.109375 to 0.109375
- w_out_pool: bfloat16 [1024, 1024], P('tp', 'fs'), may hold values from -0.109375 to 0.109375
Outputs:
- layer_out: bfloat16 [4, 16384, 1024], P('fs', ('sp', 'tp'))
The draws below stay inside these ranges and needn't reach their ends.
All inputs are finite; a program needn't handle non-finite values.
Results may differ from the reference program's by a relative error of at most 0.0075.
Values may be sent and summed in bfloat16 or wider, within the bound.
A program may use at most 128 MiB of HBM per device.

```python
import math
import jax
import jax.numpy as jnp
from jax import lax

D = 1024
MIXER_HEADS = 32
HEAD_DIM = 64
GROUPS = 4
STATE = 128
POOL_DIM = 256
POOL_GROUPS = 4
CONV = 5
BLOCK = 128
GRID_W = 32
TOK_DEV = 256
INNER = 2048
POOL = 1024
SEQUENCE_LENGTH = 16384
SEQUENCE_COUNT = 4
N_TP = 2


def draw_rate_log(key, part):
    pick_key, rapid_random_key, gentle_key = jax.random.split(jax.random.fold_in(key, 7), 3)
    fast_share = 0.5
    chosen = jax.random.uniform(pick_key, (2, MIXER_HEADS), jnp.float32) < fast_share
    quick = jax.random.uniform(rapid_random_key, (2, MIXER_HEADS), jnp.float32, math.log(1.0 / 80.0), math.log(1.0 / 25.0))
    gentle = jax.random.uniform(gentle_key, (2, MIXER_HEADS), jnp.float32, math.log(0.05), math.log(0.25)) - math.log(SEQUENCE_LENGTH)
    return jnp.where(chosen, quick, gentle).astype(jnp.float32)


def draw_decay_extra(key, part):
    level_key, position_random_key, depth_random_key, count_random_key = jax.random.split(jax.random.fold_in(key, 13), 4)
    devices_along = SEQUENCE_LENGTH // TOK_DEV
    spike_slot_list = 12
    level_low = 0.05
    level_high = 5.0
    retained_lower = 0.4
    retained_upper = 0.8
    levels = jnp.exp(jax.random.uniform(level_key, (SEQUENCE_COUNT, devices_along, 1, 2, MIXER_HEADS), jnp.float32, math.log(level_low), math.log(level_high)))
    steady_level = jnp.broadcast_to(levels, (SEQUENCE_COUNT, devices_along, TOK_DEV, 2, MIXER_HEADS)).reshape(SEQUENCE_COUNT, SEQUENCE_LENGTH, 2, MIXER_HEADS) * (-1.0 / SEQUENCE_LENGTH)
    spike_positions = jax.random.randint(position_random_key, (SEQUENCE_COUNT, spike_slot_list, 2, MIXER_HEADS), 0, SEQUENCE_LENGTH)
    spike_counts = jax.random.randint(count_random_key, (SEQUENCE_COUNT, 1, 2, MIXER_HEADS), 0, spike_slot_list + 1)
    retained_fraction = jax.random.uniform(depth_random_key, (SEQUENCE_COUNT, spike_slot_list, 2, MIXER_HEADS), jnp.float32, retained_lower, retained_upper)
    slot_ranking = jnp.arange(spike_slot_list, dtype=jnp.int32)[None, :, None, None]
    spike_logarithms = jnp.where(slot_ranking < spike_counts, jnp.log(retained_fraction), 0.0)
    sequence_number = jnp.broadcast_to(jnp.arange(SEQUENCE_COUNT, dtype=jnp.int32)[:, None, None, None], spike_positions.shape)
    direction_number = jnp.broadcast_to(jnp.arange(2, dtype=jnp.int32)[None, None, :, None], spike_positions.shape)
    head_number = jnp.broadcast_to(jnp.arange(MIXER_HEADS, dtype=jnp.int32)[None, None, None, :], spike_positions.shape)
    spike_events = jnp.zeros((SEQUENCE_COUNT, SEQUENCE_LENGTH, 2, MIXER_HEADS), jnp.float32).at[sequence_number, spike_positions, direction_number, head_number].min(spike_logarithms)
    return (steady_level + spike_events).astype(jnp.float32)


def level_of(rng, dims, cuts, least, top_value):
    gain, own = 1.0, jax.random.fold_in(rng, 6)
    for axis_at, parts in cuts:
        heights = jnp.exp(jax.random.uniform(jax.random.fold_in(own, axis_at), (parts,), jnp.float32, least / len(cuts), top_value / len(cuts)))
        gain = gain * jnp.repeat(heights, dims[axis_at] // parts).reshape([-1 if axis == axis_at else 1 for axis in range(len(dims))])
    return gain


def gaussian(own_key, shape, spread, reach, cuts=(), kind=jnp.bfloat16):
    level = level_of(own_key, shape, cuts, -0.22, 0.18) if cuts else 1.0
    values = jax.random.normal(own_key, shape, jnp.float32) * spread * level
    return jnp.minimum(jnp.maximum(values, -reach), reach).astype(kind)


def setup_inputs(seed: int = 0) -> dict:
    streams_of = jax.random.split(jax.random.key(seed), 17)
    tokens = gaussian(streams_of[0], (SEQUENCE_COUNT, SEQUENCE_LENGTH, D), 1.0, 6.0, ((0, 4), (1, 64), (2, 2)))
    w_inner = gaussian(streams_of[1], (D, INNER), D ** -0.5, 0.1875, ((0, 64), (1, 2)))
    w_gate = gaussian(streams_of[2], (D, INNER), D ** -0.5, 0.1875, ((0, 64), (1, 2)))
    w_write = gaussian(streams_of[3], (D, GROUPS * STATE), D ** -0.5, 0.1875, ((0, 64), (1, 2)))
    w_read = gaussian(streams_of[4], (D, GROUPS * STATE), D ** -0.5, 0.1875, ((0, 64), (1, 2)))
    w_pool_in = gaussian(streams_of[5], (D, POOL), D ** -0.5, 0.1875, ((0, 64), (1, 2)))
    w_step = gaussian(streams_of[6], (D, 2, MIXER_HEADS), D ** -0.5, 0.1875)
    conv_inner = gaussian(streams_of[7], (CONV, INNER), CONV ** -0.5, 2.5)
    conv_cross = gaussian(streams_of[8], (CONV, 2, GROUPS * STATE), CONV ** -0.5, 2.5)
    rate_log = draw_rate_log(jax.random.fold_in(streams_of[16], 71), 0)
    decay_extra = draw_decay_extra(jax.random.fold_in(streams_of[16], 71), 0)
    norm_gain = jnp.clip(1.0 + 0.18 * jax.random.normal(streams_of[11], (INNER,), jnp.float32), 0.1, 1.9)
    pool_mix = gaussian(streams_of[12], (POOL_GROUPS, POOL_DIM, POOL_DIM), POOL_DIM ** -0.5, 0.375)
    pool_gain = jnp.clip(1.0 + 0.18 * jax.random.normal(streams_of[13], (POOL,), jnp.float32), 0.1, 1.9)
    w_out_inner = gaussian(streams_of[14], (INNER, D), (MIXER_HEADS * HEAD_DIM + POOL_GROUPS * POOL_DIM) ** -0.5, 0.109375, ((0, 2), (1, 4)))
    w_out_pool = gaussian(streams_of[15], (POOL, D), (MIXER_HEADS * HEAD_DIM + POOL_GROUPS * POOL_DIM) ** -0.5, 0.109375, ((0, 2), (1, 4)))
    return {"tokens": tokens, "w_inner": w_inner, "w_gate": w_gate, "w_write": w_write, "w_read": w_read, "w_pool_in": w_pool_in, "w_step": w_step, "conv_inner": conv_inner, "conv_cross": conv_cross, "rate_log": rate_log, "decay_extra": decay_extra, "norm_gain": norm_gain, "pool_mix": pool_mix, "pool_gain": pool_gain, "w_out_inner": w_out_inner, "w_out_pool": w_out_pool}


HIGHEST = lax.Precision.HIGHEST
EPSILON = 1e-05

def centred_taps(streams, conv_taps):
    half_width = conv_taps.shape[0] // 2
    length = streams.shape[0]
    padded = jnp.pad(streams, ((half_width, half_width), (0, 0)))
    running = jnp.zeros_like(streams)
    for offset in range(conv_taps.shape[0]):
        running = running + padded[offset:offset + length] * conv_taps[offset]
    return running

def state_pass(values, decays, writer_rows, read_rows):
    length = decays.shape[0]
    blocks = length // BLOCK
    per_group = MIXER_HEADS // GROUPS
    lower_mask = jnp.tril(jnp.ones((BLOCK, BLOCK), dtype=bool))[:, :, None]

    def to_blocks(array):
        return array.reshape((blocks, BLOCK) + array.shape[1:])

    def advance(carried, pieces):
        block_values, block_decays, block_writes, block_reads = pieces
        cumulative = jnp.cumsum(block_decays, axis=0)
        segment_log = cumulative[:, None, :] - cumulative[None, :, :]
        weights = jnp.exp(jnp.where(lower_mask, segment_log, -jnp.inf))
        scores = jnp.einsum('ign,jgn->ijg', block_reads, block_writes, precision=HIGHEST)
        scores = jnp.repeat(scores, per_group, axis=2)
        inside = jnp.einsum('ijh,jhp->ihp', scores * weights, block_values, precision=HIGHEST)
        reads_head = jnp.repeat(block_reads, per_group, axis=1)
        carried_out = jnp.einsum('ihn,hpn->ihp', reads_head, carried, precision=HIGHEST) * jnp.exp(cumulative)[:, :, None]
        tail_decay = jnp.exp(cumulative[-1:] - cumulative)
        writes_head = jnp.repeat(block_writes, per_group, axis=1)
        fresh = jnp.einsum('jhn,jhp->hpn', writes_head * tail_decay[:, :, None], block_values, precision=HIGHEST)
        carried = carried * jnp.exp(cumulative[-1])[:, None, None] + fresh
        return (carried, inside + carried_out)
    zero_state = jnp.zeros((MIXER_HEADS, HEAD_DIM, STATE), jnp.float32)
    last_state, outputs = lax.scan(advance, zero_state, (to_blocks(values), to_blocks(decays), to_blocks(writer_rows), to_blocks(read_rows)))
    return outputs.reshape(length, MIXER_HEADS, HEAD_DIM)

def window_sum(values, mesh_direction, window):
    extent = values.shape[mesh_direction]
    widths = [(0, 0)] * values.ndim
    widths[mesh_direction] = (1, 0)
    running = jnp.cumsum(jnp.pad(values, widths), axis=mesh_direction)
    places = jnp.arange(extent).astype(jnp.int32)
    lower_end = jnp.clip(places - window // 2, 0, extent).astype(jnp.int32)
    upper_end = jnp.clip(places - window // 2 + window, 0, extent).astype(jnp.int32)
    summed = jnp.take(running, upper_end, axis=mesh_direction) - jnp.take(running, lower_end, axis=mesh_direction)
    return (summed, (upper_end - lower_end).astype(jnp.float32))

def pool_mixer(pool_in, pool_mix, pool_gain):
    grid_rows = pool_in.shape[0] // GRID_W
    grid = pool_in.astype(jnp.float32).reshape(grid_rows, GRID_W, POOL_GROUPS, POOL_DIM)
    results = []
    for group_index in range(POOL_GROUPS):
        window = 2 ** (group_index + 1)
        channel_plane = grid[:, :, group_index]
        summed, row_counts = window_sum(channel_plane, 0, window)
        summed, col_counts = window_sum(summed, 1, window)
        average = summed / (row_counts[:, None, None] * col_counts[None, :, None])
        offsets = (average - channel_plane).astype(jnp.bfloat16).reshape(-1, POOL_DIM)
        mixed_rows = jnp.dot(offsets, pool_mix[group_index], preferred_element_type=jnp.float32)
        gain_part = pool_gain[group_index * POOL_DIM:(group_index + 1) * POOL_DIM]
        results.append((mixed_rows * gain_part).astype(jnp.bfloat16))
    return jnp.concatenate(results, axis=1)

def one_sequence(tokens, decay_extra, weights):
    w_inner, w_gate, w_write, w_read, w_pool_in, w_step, conv_inner, conv_cross, rate_log, norm_gain, pool_mix, pool_gain, w_out_inner, w_out_pool = weights
    length = tokens.shape[0]
    cross_width = GROUPS * STATE
    inner_x = jnp.dot(tokens, w_inner, preferred_element_type=jnp.float32).astype(jnp.bfloat16)
    gate_in = jnp.dot(tokens, w_gate, preferred_element_type=jnp.float32).astype(jnp.bfloat16)
    write_in = jnp.dot(tokens, w_write, preferred_element_type=jnp.float32).astype(jnp.bfloat16)
    read_in = jnp.dot(tokens, w_read, preferred_element_type=jnp.float32).astype(jnp.bfloat16)
    pool_in = jnp.dot(tokens, w_pool_in, preferred_element_type=jnp.float32).astype(jnp.bfloat16)
    raw_step = jnp.dot(tokens, w_step.reshape(D, 2 * MIXER_HEADS), preferred_element_type=jnp.float32).reshape(length, 2, MIXER_HEADS)
    streams = jnp.concatenate([inner_x, write_in, read_in], axis=1).astype(jnp.float32)
    conv_taps = jnp.concatenate([conv_inner, conv_cross[:, 0], conv_cross[:, 1]], axis=1).astype(jnp.float32)
    activated = jax.nn.silu(centred_taps(streams, conv_taps))
    values = activated[:, :INNER].reshape(length, MIXER_HEADS, HEAD_DIM)
    writer_rows = activated[:, INNER:INNER + cross_width].reshape(length, GROUPS, STATE)
    read_rows = activated[:, INNER + cross_width:].reshape(length, GROUPS, STATE)
    step_size = jax.nn.softplus(raw_step)
    log_decay = -step_size * jnp.exp(rate_log)[None] + decay_extra
    forward = state_pass(values * step_size[:, 0, :, None], log_decay[:, 0], writer_rows, read_rows)
    backward = state_pass((values * step_size[:, 1, :, None])[::-1], log_decay[::-1, 1], writer_rows[::-1], read_rows[::-1])[::-1]
    gated_out = (forward + backward) * jax.nn.silu(gate_in.astype(jnp.float32)).reshape(length, MIXER_HEADS, HEAD_DIM)
    rms_scale = lax.rsqrt(lax.optimization_barrier(jnp.mean(gated_out * gated_out, axis=2, keepdims=True)) + EPSILON)
    mixer_out = (gated_out * rms_scale * norm_gain.reshape(MIXER_HEADS, HEAD_DIM)).reshape(length, INNER).astype(jnp.bfloat16)
    pooled = pool_mixer(pool_in, pool_mix, pool_gain)
    inner_part = INNER // N_TP
    pool_part = POOL // N_TP
    summed = jnp.zeros((length, D), jnp.float32)
    for tp_rank in range(N_TP):
        inner_cols = slice(tp_rank * inner_part, (tp_rank + 1) * inner_part)
        pool_cols = slice(tp_rank * pool_part, (tp_rank + 1) * pool_part)
        partial_value = jnp.dot(mixer_out[:, inner_cols], w_out_inner[inner_cols], preferred_element_type=jnp.float32)
        partial_value = partial_value + jnp.dot(pooled[:, pool_cols], w_out_pool[pool_cols], preferred_element_type=jnp.float32)
        rounded = lax.optimization_barrier(partial_value.astype(jnp.bfloat16))
        summed = summed + rounded.astype(jnp.float32)
    return summed.astype(jnp.bfloat16)

def reference(tokens, w_inner, w_gate, w_write, w_read, w_pool_in, w_step, conv_inner, conv_cross, rate_log, decay_extra, norm_gain, pool_mix, pool_gain, w_out_inner, w_out_pool):
    weights = (w_inner, w_gate, w_write, w_read, w_pool_in, w_step, conv_inner, conv_cross, rate_log, norm_gain, pool_mix, pool_gain, w_out_inner, w_out_pool)

    def run_sequence(sequence_pair):
        return one_sequence(sequence_pair[0], sequence_pair[1], weights)
    return lax.map(run_sequence, (tokens, decay_extra))
```

```python
import functools

import jax
import jax.numpy as jnp
from jax import lax
from jax.experimental import pallas as pl
from jax.experimental.pallas import tpu as pltpu
from jax.sharding import Mesh
from jax.sharding import PartitionSpec as P

MESH = pl.DeviceIdType.MESH
F32, BF16 = jnp.float32, jnp.bfloat16
HIGHEST = lax.Precision.HIGHEST
SP = ("z", "y")
EPSILON = 1e-05
T = 256
GRID_W = 32


def dot(a, b, dims=((1,), (0,)), **kw):
    return lax.dot_general(a, b, (dims, ((), ())), preferred_element_type=F32, **kw)


def kernel(
    tok, w_inner, w_gate, w_write, w_read, w_pool, wstep, par, rate, dec_in, pmix_in, woi_in, wop_in,
    out,
    x_b, hrow, hall, wa, wb, woi, wop, de, pmix, p_s, hp, y_s, c_s, ea, er, gate, pool, m_s,
    st, dec, r1, d1, r2, d2, res, tot, totd, inc, own, dsend, drecv, xsend, xrecv, mix_s, pld_s,
    lsem, ssem, rsem,
):
    z, y, f, t = (lax.axis_index(a) for a in ("z", "y", "fs", "tp"))
    sp = z * 8 + y
    nxt, prv = lax.rem(sp + 1, 64), lax.rem(sp + 63, 64)
    nxt = {"z": nxt // 8, "y": lax.rem(nxt, 8)}
    prv = {"z": prv // 8, "y": lax.rem(prv, 8)}
    half = f // 2
    counter = [0]
    sent = []

    def send(src, dst, dev):
        i = counter[0]
        counter[0] += 1
        c = pltpu.make_async_remote_copy(
            src_ref=src, dst_ref=dst, send_sem=ssem.at[i], recv_sem=rsem.at[i],
            device_id=dev, device_id_type=MESH,
        )
        c.start()
        sent.append(c)
        return c

    def ymod(d):
        return lax.rem(y + d, 8)

    def zmod(d):
        return lax.rem(z + d, 8)

    def fmod(d):
        return lax.rem(f + d, 4)

    lcount = [0]

    def local(src, dst):
        c = pltpu.make_async_copy(src, dst, lsem.at[lcount[0]])
        lcount[0] += 1
        c.start()
        return c

    peers = [{"y": ymod(d)} for d in range(1, 8)] + [{"z": zmod(d)} for d in range(1, 8)]
    group = [{"fs": fmod(d), "tp": lax.rem(t + e, 2)} for d in range(4) for e in range(2) if d + e]
    peers += group + [nxt, prv]

    own_a, own_b = wa.at[sp], wb.at[sp]
    weights_local = [
        local(w_inner.at[:, pl.ds(pl.multiple_of(f * 256, 256), 256)], own_a.at[:, pl.ds(0, 256)]),
        local(w_write.at[:, pl.ds(pl.multiple_of(half * 128, 128), 128)], own_a.at[:, pl.ds(256, 128)]),
        local(w_read.at[:, pl.ds(pl.multiple_of(half * 128, 128), 128)], own_a.at[:, pl.ds(384, 128)]),
        local(w_gate.at[:, pl.ds(pl.multiple_of(f * 256, 256), 256)], own_b.at[:, pl.ds(0, 256)]),
        local(w_pool.at[:, pl.ds(pl.multiple_of(f * 128, 128), 128)], own_b.at[:, pl.ds(256, 128)]),
    ]
    tok_local = local(tok.at[0], x_b.at[f, t])
    others = [
        local(dec_in.at[f], de.at[f]),
        local(pmix_in.at[t * 2 + half, pl.ds(pl.multiple_of(lax.rem(f, 2) * 128, 128), 128)], pmix),
        local(woi_in.at[pl.ds(pl.multiple_of(f * 256, 256), 256)], woi.at[f]),
        local(wop_in.at[pl.ds(pl.multiple_of(half * 256, 256), 256)], wop.at[f]),
    ]
    barrier = pltpu.get_barrier_semaphore()
    for p in peers:
        pl.semaphore_signal(barrier, inc=1, device_id=p, device_id_type=MESH)
    pl.semaphore_wait(barrier, len(peers))

    tok_local.wait()
    x_own = x_b.at[f, t]
    edge_n = send(x_own.at[pl.ds(240, 16)], hrow.at[0], nxt)
    edge_p = send(x_own.at[pl.ds(0, 16)], hrow.at[1], prv)
    x_right = send(x_own, x_own, {"fs": fmod(1)})
    x_left = send(x_own, x_own, {"fs": fmod(3)})
    x_pair = [send(x_own, x_own, {"tp": 1 - t})]
    for c in weights_local:
        c.wait()
    a1 = [send(own_a, own_a, {"y": ymod(d)}) for d in (1, 7, 2, 6, 3, 5, 4)]
    b1 = [send(own_b, own_b, {"z": zmod(d)}) for d in (1, 7, 2, 6, 3, 5, 4)]

    def slab_a(k):
        return wa.at[pl.ds(pl.multiple_of(zmod(k) * 8, 8), 8)]

    edge_n.wait_recv()
    edge_p.wait_recv()
    local_halo = local(hrow, hall.at[f, t])
    halos = [send(hrow, hall.at[f, t], g) for g in group]
    for c in a1:
        c.wait_recv()
    ar = [send(slab_a(0), slab_a(0), {"z": zmod(1)})]
    al = [send(slab_a(0), slab_a(0), {"z": zmod(7)})]
    for c in b1:
        c.wait_recv()

    def cols_b(k):
        return [wb.at[zz * 8 + ymod(k)] for zz in range(8)]

    br = [[send(s, s, {"y": ymod(1)}) for s in cols_b(0)]]
    bl = [[send(s, s, {"y": ymod(7)}) for s in cols_b(0)]]

    x_right.wait_recv()
    lblk = x_b.at[fmod(3), t]
    x_fr = send(lblk.at[pl.ds(0, 128)], lblk.at[pl.ds(0, 128)], {"fs": fmod(1)})
    x_pair.append(send(lblk, lblk, {"tp": 1 - t}))
    x_left.wait_recv()
    rblk = x_b.at[fmod(1), t]
    x_fl = send(rblk.at[pl.ds(128, 128)], rblk.at[pl.ds(128, 128)], {"fs": fmod(3)})
    x_pair.append(send(rblk, rblk, {"tp": 1 - t}))
    decs = [send(dec_in.at[fmod(d)], de.at[f], {"fs": fmod(d)}) for d in (1, 3, 2)]

    for k in range(1, 4):
        ar[k - 1].wait_recv()
        ar.append(send(slab_a(8 - k), slab_a(8 - k), {"z": zmod(1)}))
        al[k - 1].wait_recv()
        if k < 3:
            al.append(send(slab_a(k), slab_a(k), {"z": zmod(7)}))
        for c in br[k - 1]:
            c.wait_recv()
        br.append([send(s, s, {"y": ymod(1)}) for s in cols_b(8 - k)])
        for c in bl[k - 1]:
            c.wait_recv()
        if k < 3:
            bl.append([send(s, s, {"y": ymod(7)}) for s in cols_b(k)])
        if k == 1:
            x_fr.wait_recv()
            x_fl.wait_recv()
            oblk = x_b.at[fmod(2), t]
            x_pair.append(send(oblk, oblk, {"tp": 1 - t}))
    wos = []
    for d in (1, 3, 2):
        g = fmod(d)
        wos.append(send(woi_in.at[pl.ds(pl.multiple_of(g * 256, 256), 256)], woi.at[f], {"fs": g}))
        wos.append(send(wop_in.at[pl.ds(pl.multiple_of((g // 2) * 256, 256), 256)], wop.at[f], {"fs": g}))
    local_halo.wait()
    for c in others:
        c.wait()
    for c in x_pair + halos + decs:
        c.wait_recv()
    ar[3].wait_recv()
    for c in br[3]:
        c.wait_recv()

    wa0, wa1 = wa[0:32].reshape(512, 512), wa[32:64].reshape(512, 512)
    h0 = hall[:, 0].reshape(128, 512)
    h1 = hall[:, 1].reshape(128, 512)
    hproj = (dot(h0, wa0) + dot(h1, wa1)).astype(BF16).astype(F32)
    side = lax.rem(lax.broadcasted_iota(jnp.int32, (128, 512), 0) // 16, 2)
    gone = jnp.logical_or(
        jnp.logical_and(side == 0, sp == 0), jnp.logical_and(side == 1, sp == 63)
    )
    hp[...] = jnp.where(gone, 0.0, hproj).reshape(4, 2, 16, 512)

    ii = lax.broadcasted_iota(jnp.int32, (T, T), 0)
    jj = lax.broadcasted_iota(jnp.int32, (T, T), 1)
    low = lax.broadcasted_iota(jnp.int32, (T, 128), 1) < 64

    def spread(cols, c):
        parts = [
            jnp.where(low, cols[:, c + 2 * q : c + 2 * q + 1], cols[:, c + 2 * q + 1 : c + 2 * q + 2])
            for q in range(2)
        ]
        return jnp.concatenate(parts, axis=1)

    def front(s, _):
        x0, x1 = x_b[s, 0], x_b[s, 1]
        pa = dot(x0, wa[0:32].reshape(512, 512)) + dot(x1, wa[32:64].reshape(512, 512))
        p_s[16:272, :] = pa.astype(BF16).astype(F32)
        p_s[0:16, :] = hp[s, 0]
        p_s[272:288, :] = hp[s, 1]
        conv = p_s[14 : 14 + T, :] * par[0:1, :]
        for j in range(1, 5):
            conv = conv + p_s[14 + j : 14 + j + T, :] * par[j : j + 1, :]
        act = conv / (1.0 + jnp.exp(-conv))
        v, b, c = act[:, 0:256], act[:, 256:384], act[:, 384:512]
        raw = dot(wstep[:, 0:512], x0, ((1,), (1,))) + dot(wstep[:, 512:1024], x1, ((1,), (1,)))
        step = jnp.maximum(raw, 0.0) + jnp.log1p(jnp.exp(-jnp.abs(raw)))
        ld = de[s] - step * rate[:, 0:1]
        pre = dot(ld, (ii <= jj).astype(F32), precision=HIGHEST)
        suf = dot(ld, (ii >= jj).astype(F32), precision=HIGHEST)
        first = lax.broadcasted_iota(jnp.int32, (8, T), 0) < 4
        cum = jnp.where(first, pre, suf)
        cols = jnp.concatenate([cum, step, jnp.zeros((112, T), F32)], axis=0).T
        bb, cb = b.astype(BF16), c.astype(BF16)
        c_s[s] = cb
        scores = dot(cb, bb, ((1,), (1,)))
        vb = v.astype(BF16)
        ys = []
        for q in range(2):
            vp = vb[:, q * 128 : (q + 1) * 128]
            pair = []
            for e in range(2):
                h = 2 * q + e
                expo = jnp.where(
                    jj <= ii,
                    cols[:, h : h + 1] - cum[h : h + 1, :],
                    cols[:, 4 + h : 5 + h] - cum[4 + h : 5 + h, :],
                )
                df, db = step[h : h + 1, :], step[4 + h : 5 + h, :]
                dts = jnp.where(jj < ii, df, jnp.where(jj > ii, db, df + db))
                pair.append(dot((scores * jnp.exp(expo) * dts).astype(BF16), vp))
            ys.append(jnp.where(low, pair[0], pair[1]))
        y_s[s] = jnp.concatenate(ys, axis=1)
        bt = b.T.astype(BF16)
        ex_a, ex_r = spread(cols, 0), spread(cols, 4)
        end_a, end_r = ex_a[T - 1 : T, :], ex_r[0:1, :]
        vf = (v * (jnp.exp(end_a - ex_a) * spread(cols, 8))).astype(BF16)
        vr = (v * (jnp.exp(end_r - ex_r) * spread(cols, 12))).astype(BF16)
        st[:, 2 * s] = dot(bt, vf).astype(BF16).reshape(8, 16, 256)
        st[:, 2 * s + 1] = dot(bt, vr).astype(BF16).reshape(8, 16, 256)
        dec[2 * s] = jnp.broadcast_to(end_a, (8, 256))
        dec[2 * s + 1] = jnp.broadcast_to(end_r, (8, 256))
        ea[s] = jnp.exp(ex_a)
        er[s] = jnp.exp(ex_r)
        pb = dot(x0, wb[0:32].reshape(512, 384)) + dot(x1, wb[32:64].reshape(512, 384))
        pb = pb.astype(BF16)
        g = pb[:, 0:256].astype(F32)
        gate[s] = g / (1.0 + jnp.exp(-g))
        pool[1, s] = pb[:, 256:384]
        return _

    lax.fori_loop(0, 4, front, 0)

    own_st = local(st.at[y], r1.at[y])
    own_dec = local(dec, d1.at[y])
    s1 = []
    for d in (1, 7, 2, 6, 3, 5, 4):
        s1.append(send(st.at[ymod(d)], r1.at[y], {"y": ymod(d)}))
        s1.append(send(dec, d1.at[y], {"y": ymod(d)}))
    pool_n = send(pool.at[1], pool.at[0], nxt)
    pool_p = send(pool.at[1], pool.at[2], prv)

    g_index = t * 2 + half
    k = jnp.left_shift(jnp.int32(2), g_index)
    ti = lax.broadcasted_iota(jnp.int32, (T, 3 * T), 0)
    tj = lax.broadcasted_iota(jnp.int32, (T, 3 * T), 1)
    ri, ci = ti // GRID_W + 8, ti % GRID_W
    rj, cj = tj // GRID_W, tj % GRID_W
    grow = rj + (sp * 8 - 8)
    inside = (rj >= ri - k // 2) & (rj < ri + k // 2) & (cj >= ci - k // 2) & (cj < ci + k // 2)
    inside = inside & (grow >= 0) & (grow < 512)
    m_s[...] = inside.astype(F32).astype(BF16)

    own_st.wait()
    own_dec.wait()
    for c in s1:
        c.wait_recv()
    for n in range(8):
        run = jnp.zeros((16, 256), F32)
        cumd = jnp.zeros((8, 256), F32)
        for i in range(8) if n % 2 == 0 else reversed(range(8)):
            res[i, n] = run
            tot_d = d1[i, n]
            totd_prev = cumd
            d1[i, n] = totd_prev
            w = jnp.exp(tot_d)
            run = run * jnp.concatenate([w, w], axis=0) + r1[i, n].astype(F32)
            cumd = cumd + tot_d
        tot[n] = run.astype(BF16)
        totd[n] = cumd
    own_t = local(tot, r2.at[z])
    own_td = local(totd, d2.at[z])
    s2 = []
    for d in (1, 7, 2, 6, 3, 5, 4):
        s2.append(send(tot, r2.at[z], {"z": zmod(d)}))
        s2.append(send(totd, d2.at[z], {"z": zmod(d)}))
    own_t.wait()
    own_td.wait()
    for c in s2:
        c.wait_recv()
    for n in range(8):
        acc = jnp.zeros((16, 256), F32)
        for i in range(8) if n % 2 == 0 else reversed(range(8)):
            w = jnp.exp(d2[i, n])
            new = acc * jnp.concatenate([w, w], axis=0) + r2[i, n].astype(F32)
            used = (i < z) if n % 2 == 0 else (i > z)
            acc = jnp.where(used, new, acc)
        for i in range(8):
            w = jnp.exp(d1[i, n])
            r1[i, n] = (res[i, n] + acc * jnp.concatenate([w, w], axis=0)).astype(BF16)
    own_i = local(r1.at[y], inc.at[y])
    s3 = [send(r1.at[ymod(d)], inc.at[y], {"y": ymod(d)}) for d in (1, 7, 2, 6, 3, 5, 4)]

    pool_n.wait_recv()
    pool_p.wait_recv()
    ti1 = lax.broadcasted_iota(jnp.int32, (T, 128), 0)
    row = ti1 // GRID_W + sp * 8
    col = ti1 % GRID_W
    count = (
        (jnp.minimum(row + k // 2, 512) - jnp.maximum(row - k // 2, 0))
        * (jnp.minimum(col + k // 2, GRID_W) - jnp.maximum(col - k // 2, 0))
    ).astype(F32)

    def pools(s, _):
        rows = jnp.concatenate([pool[0, s], pool[1, s], pool[2, s]], axis=0)
        off = dot(m_s[...], rows) / count - pool[1, s].astype(F32)
        mixed = dot(off.astype(BF16), pmix[...]) * par[5:6, 256:512]
        pld_s[s] = mixed.astype(BF16)
        return _

    lax.fori_loop(0, 4, pools, 0)

    own_i.wait()
    for c in s3:
        c.wait_recv()
    for c in wos:
        c.wait_recv()

    blk = (ii // 64 == jj // 64).astype(F32) * (1.0 / 64.0)
    blk = blk.astype(BF16)

    def finish(s):
        cb = c_s[s]
        carried = dot(cb, inc[:, 2 * s].reshape(128, 256)) * ea[s]
        carried = carried + dot(cb, inc[:, 2 * s + 1].reshape(128, 256)) * er[s]
        g = (y_s[s] + carried) * gate[s]
        ms = dot((g * g).astype(BF16), blk)
        mix_s[...] = (g * lax.rsqrt(ms + EPSILON) * par[5:6, 0:256]).astype(BF16)

    pair, far = [], []
    order = [fmod(2), fmod(1), fmod(3), f]
    mine = pl.ds(pl.multiple_of(t * 128, 128), 128)
    theirs = pl.ds(pl.multiple_of((1 - t) * 128, 128), 128)
    for o in range(4):
        s = order[o]
        finish(s)
        for q in range(4):
            cs = slice(q * 256, (q + 1) * 256)
            part = dot(mix_s[theirs, :], woi[q]) + dot(pld_s[s, theirs, :], wop[q])
            dsend[o, :, cs] = part.astype(BF16)
        pair.append((send(dsend.at[o], drecv.at[s], {"tp": 1 - t})))
        for q in range(4):
            cs = slice(q * 256, (q + 1) * 256)
            own[o, :, cs] = dot(mix_s[mine, :], woi[q]) + dot(pld_s[s, mine, :], wop[q])
        pair[o].wait_recv()
        chip = own[o] + drecv[s].astype(F32)
        if o < 3:
            xsend[o] = chip.astype(BF16)
            far.append(send(xsend.at[o], xrecv.at[o], {"fs": s}))
        else:
            own[o] = chip
    for c in far:
        c.wait_recv()
    total = own[3] + xrecv[0].astype(F32) + xrecv[1].astype(F32) + xrecv[2].astype(F32)
    out[0] = total.astype(BF16)
    for c in sent:
        c.wait_send()


N_REMOTE = 160


def body(
    tokens, w_inner, w_gate, w_write, w_read, w_pool_in, w_step, conv_inner, conv_cross, rate_log,
    decay_extra, norm_gain, pool_mix, pool_gain, w_out_inner, w_out_pool,
):
    f, t = lax.axis_index("fs"), lax.axis_index("tp")
    group = t * 2 + f // 2
    h0 = t * 16 + f * 4
    cut = lax.dynamic_slice_in_dim
    wstep = cut(w_step, h0, 4, 2).reshape(1024, 8).T
    taps = jnp.concatenate(
        [
            cut(conv_inner, h0 * 64, 256, 1),
            cut(conv_cross[:, 0], group * 128, 128, 1),
            cut(conv_cross[:, 1], group * 128, 128, 1),
        ],
        axis=1,
    ).astype(F32)
    gains = jnp.concatenate([cut(norm_gain, h0 * 64, 256, 0), cut(pool_gain, group * 256, 256, 0)])
    par = jnp.concatenate([taps, gains[None], jnp.zeros((2, 512), F32)], axis=0)
    rate = jnp.broadcast_to(jnp.exp(cut(rate_log, h0, 4, 1)).reshape(8, 1), (8, 128))
    dec = jnp.transpose(decay_extra[0].reshape(T, 2, 4, 4), (2, 1, 3, 0)).reshape(4, 8, T)
    any_spec = pl.BlockSpec(memory_space=pl.ANY)
    vm = pl.BlockSpec(memory_space=pltpu.VMEM)
    V = pltpu.VMEM
    scratch = [
        V((4, 2, T, 512), BF16),
        V((2, 16, 512), BF16),
        V((4, 2, 2, 16, 512), BF16),
        V((64, 16, 512), BF16),
        V((64, 16, 384), BF16),
        V((4, 256, 256), BF16),
        V((4, 256, 256), BF16),
        V((4, 8, T), F32),
        V((128, 256), BF16),
        V((288, 512), F32),
        V((4, 2, 16, 512), F32),
        V((4, T, 256), F32),
        V((4, T, 128), BF16),
        V((4, T, 256), F32),
        V((4, T, 256), F32),
        V((4, T, 256), F32),
        V((3, 4, T, 128), BF16),
        V((T, 3 * T), BF16),
        V((8, 8, 16, 256), BF16),
        V((8, 8, 256), F32),
        V((8, 8, 16, 256), BF16),
        V((8, 8, 8, 256), F32),
        V((8, 8, 16, 256), BF16),
        V((8, 8, 8, 256), F32),
        V((8, 8, 16, 256), F32),
        V((8, 16, 256), BF16),
        V((8, 8, 256), F32),
        V((8, 8, 16, 256), BF16),
        V((4, 128, 1024), F32),
        V((4, 128, 1024), BF16),
        V((4, 128, 1024), BF16),
        V((3, 128, 1024), BF16),
        V((3, 128, 1024), BF16),
        V((T, 256), BF16),
        V((4, T, 256), BF16),
        pltpu.SemaphoreType.DMA((20,)),
        pltpu.SemaphoreType.DMA((N_REMOTE,)),
        pltpu.SemaphoreType.DMA((N_REMOTE,)),
    ]
    return pl.pallas_call(
        kernel,
        out_shape=jax.ShapeDtypeStruct((1, 128, 1024), BF16),
        in_specs=[any_spec] * 6 + [vm, vm, vm] + [any_spec] * 4,
        out_specs=vm,
        scratch_shapes=scratch,
        compiler_params=pltpu.CompilerParams(
            collective_id=0, has_side_effects=True, vmem_limit_bytes=60 * 1024 * 1024
        ),
    )(
        tokens, w_inner, w_gate, w_write, w_read, w_pool_in, wstep, par, rate, dec, pool_mix,
        w_out_inner, w_out_pool,
    )


def solution(mesh):
    finer = Mesh(
        mesh.devices.reshape(8, 8, mesh.shape["fs"], mesh.shape["tp"]), ("z", "y", "fs", "tp")
    )
    in_specs = (
        P("fs", SP, "tp"),
        P(SP, "tp"),
        P(SP, "tp"),
        P(SP, "tp"),
        P(SP, "tp"),
        P(SP, "tp"),
        P(),
        P(),
        P(),
        P(),
        P("fs", SP, None, "tp"),
        P(),
        P(),
        P(),
        P("tp", "fs"),
        P("tp", "fs"),
    )
    out_specs = P("fs", ("z", "y", "tp"), None)
    return jax.shard_map(body, mesh=finer, in_specs=in_specs, out_specs=out_specs, check_vma=False)
```

```python
import functools

import jax
import jax.numpy as jnp
from jax import lax
from jax.experimental import pallas as pl
from jax.experimental.pallas import tpu as pltpu
from jax.sharding import Mesh
from jax.sharding import PartitionSpec as P

MESH = pl.DeviceIdType.MESH
F32, BF16 = jnp.float32, jnp.bfloat16
SP = ("z", "y")
EPSILON = 1e-05
T = 256
GRID_W = 32


def silu(v):
    return (0.5 * v) * (1.0 + jnp.tanh(0.5 * v))


def dot(a, b, dims=((1,), (0,)), **kw):
    return lax.dot_general(a, b, (dims, ((), ())), preferred_element_type=F32, **kw)


def kernel(
    tok, w_inner, w_gate, w_write, w_read, w_pool, wst_in, ci_in, cc_in, rate_in, dec_in, ng_in, pmix_in,
    pg_in, woi_in, wop_in,
    out,
    x_b, hrow, hall, wa1, wa2, wb1, wb2, woi, wop, de, pmix, wst, ci, cc, ng, pg, par,
    p_s, hp, y_s, v_s, b_s, c_s, cum_s, stp_s, cols_s, gate, pool, m_s,
    st, dec, r1, d1, pd, r2, d2, totd, res, tot, inc, own, dsend, drecv, raws, rawr, xsend, xrecv,
    mix_s, pld_s,
    lsem, ssem, rsem, psem,
):
    z, y, f, t = (lax.axis_index(a) for a in ("z", "y", "fs", "tp"))
    sp = z * 8 + y
    nxt, prv = lax.rem(sp + 1, 64), lax.rem(sp + 63, 64)
    nxt = {"z": nxt // 8, "y": lax.rem(nxt, 8)}
    prv = {"z": prv // 8, "y": lax.rem(prv, 8)}
    half = f // 2
    group_at = t * 2 + half
    count = [0, 0]
    sent = []

    def send(src, dst, dev):
        i = count[0]
        count[0] += 1
        c = pltpu.make_async_remote_copy(
            src_ref=src, dst_ref=dst, send_sem=ssem.at[i], recv_sem=rsem.at[i],
            device_id=dev, device_id_type=MESH,
        )
        c.start()
        sent.append(c)
        return c

    def local(src, dst):
        c = pltpu.make_async_copy(src, dst, lsem.at[count[1]])
        count[1] += 1
        c.start()
        return c

    def ymod(d):
        return lax.rem(y + d, 8)

    def zmod(d):
        return lax.rem(z + d, 8)

    def fmod(d):
        return lax.rem(f + d, 4)

    def at(v, n):
        return pl.ds(pl.multiple_of(v * n, n), n)

    near_first = (1, 7, 2, 6, 3, 5, 4)
    group = [{"fs": fmod(d), "tp": lax.rem(t + e, 2)} for d in range(4) for e in range(2) if d + e]
    peers = [{"y": ymod(d)} for d in range(1, 8)] + [{"z": zmod(d)} for d in range(1, 8)]
    peers += group + [nxt, prv]
    pair = {"tp": 1 - t}

    pool[0] = jnp.zeros((4, T, 128), BF16)
    pool[2] = jnp.zeros((4, T, 128), BF16)
    barrier = pltpu.get_barrier_semaphore()
    for p in peers:
        pl.semaphore_signal(barrier, inc=1, device_id=p, device_id_type=MESH)
    mine1, mine2, mine3, mine4 = (w.at[z, y] for w in (wa1, wa2, wb1, wb2))
    tok_local = local(tok.at[0], x_b.at[f, t])
    w_local = [
        local(w_inner.at[:, at(f, 256)], mine1),
        local(w_write.at[:, at(half, 128)], mine2.at[:, pl.ds(0, 128)]),
        local(w_read.at[:, at(half, 128)], mine2.at[:, pl.ds(128, 128)]),
        local(w_gate.at[:, at(f, 256)], mine3),
        local(w_pool.at[:, at(f, 128)], mine4),
    ]
    others = [
        local(wst_in.at[:, at(t, 16)], wst),
        local(dec_in.at[:, at(half, 8)], de.at[f]),
        local(ci_in.at[:, at(t * 4 + f, 256)], ci),
        local(cc_in.at[:, :, at(group_at, 128)], cc),
        local(ng_in, ng),
        local(pg_in, pg),
        local(pmix_in.at[group_at, at(lax.rem(f, 2), 128)], pmix),
        local(woi_in.at[at(f, 256)], woi.at[f]),
        local(wop_in.at[at(half, 256)], wop.at[f]),
    ]
    tok_local.wait()
    for c in w_local:
        c.wait()
    pl.semaphore_wait(barrier, len(peers))

    x_own = x_b.at[f, t]
    edge_n = send(x_own.at[pl.ds(240, 16)], hrow.at[0], nxt)
    edge_p = send(x_own.at[pl.ds(0, 16)], hrow.at[1], prv)
    first = [send(mine1, mine1, {"y": ymod(d)}) for d in near_first]
    second = [send(mine2, mine2, {"z": zmod(d)}) for d in near_first]
    x_right = send(x_own, x_own, {"fs": fmod(1)})
    x_left = send(x_own, x_own, {"fs": fmod(3)})
    x_pair = [send(x_own, x_own, pair)]
    decs = [send(dec_in.at[:, at(fmod(d) // 2, 8)], de.at[f], {"fs": fmod(d)}) for d in (1, 3, 2)]
    third = [send(mine3, mine3, {"y": ymod(d)}) for d in near_first]
    fourth = [send(mine4, mine4, {"z": zmod(d)}) for d in near_first]

    def ring_z(w, k, to):
        s = w.at[zmod(8 - k if to == 1 else k)]
        return send(s, s, {"z": zmod(to)})

    def ring_y(w, k, to):
        s = w.at[:, ymod(8 - k if to == 1 else k)]
        return send(s, s, {"y": ymod(to)})

    for c in first:
        c.wait_recv()
    zr, zl = [ring_z(wa1, 0, 1)], [ring_z(wa1, 0, 7)]
    for c in second:
        c.wait_recv()
    yr, yl = [ring_y(wa2, 0, 1)], [ring_y(wa2, 0, 7)]
    edge_n.wait_recv()
    edge_p.wait_recv()
    halo_local = local(hrow, hall.at[f, t])
    halos = [send(hrow, hall.at[f, t], g) for g in group]

    def step(k):
        zr[k - 1].wait_recv()
        zr.append(ring_z(wa1, k, 1))
        zl[k - 1].wait_recv()
        if k < 3:
            zl.append(ring_z(wa1, k, 7))
        yr[k - 1].wait_recv()
        yr.append(ring_y(wa2, k, 1))
        yl[k - 1].wait_recv()
        if k < 3:
            yl.append(ring_y(wa2, k, 7))

    step(1)
    x_right.wait_recv()
    block = x_b.at[fmod(3), t]
    x_fr = send(block.at[pl.ds(0, 128)], block.at[pl.ds(0, 128)], {"fs": fmod(1)})
    x_pair.append(send(block, block, pair))
    x_left.wait_recv()
    block = x_b.at[fmod(1), t]
    x_fl = send(block.at[pl.ds(128, 128)], block.at[pl.ds(128, 128)], {"fs": fmod(3)})
    x_pair.append(send(block, block, pair))
    step(2)
    for c in others:
        c.wait()
    par[0:5, 0:256] = ci[...].astype(F32)
    par[0:5, 256:384] = cc[:, 0, :].astype(F32)
    par[0:5, 384:512] = cc[:, 1, :].astype(F32)
    x_fr.wait_recv()
    x_fl.wait_recv()
    block = x_b.at[fmod(2), t]
    x_pair.append(send(block, block, pair))
    step(3)
    for c in third + fourth:
        c.wait_recv()
    gzr, gzl = [ring_z(wb1, 0, 1)], [ring_z(wb1, 0, 7)]
    gyr, gyl = [ring_y(wb2, 0, 1)], [ring_y(wb2, 0, 7)]

    def gate_step(k):
        for ring, w, make, to in ((gzr, wb1, ring_z, 1), (gyr, wb2, ring_y, 1), (gzl, wb1, ring_z, 7), (gyl, wb2, ring_y, 7)):
            if to == 1 or k < 4:
                ring[k - 1].wait_recv()
            if k < (4 if to == 1 else 3):
                ring.append(make(w, k, to))

    for c in x_pair + decs:
        c.wait_recv()
    ii = lax.broadcasted_iota(jnp.int32, (T, T), 0)
    jj = lax.broadcasted_iota(jnp.int32, (T, T), 1)
    low = lax.broadcasted_iota(jnp.int32, (T, 128), 1) < 64

    def slot_seq(o):
        return lax.rem(f + lax.rem(2 + 3 * o + (3 * o * (o - 1)) // 2, 4), 4)

    r8 = lax.broadcasted_iota(jnp.int32, (8, 1), 0)
    rate = jnp.zeros((8, 1), F32)
    for i in range(8):
        rate = jnp.where(r8 == i, rate_in[i // 4, t * 16 + f * 4 + i % 4], rate)
    rate = jnp.exp(rate)
    def pick(rows, which, n):
        chosen = rows[0:4]
        for i in range(1, n):
            chosen = jnp.where(which == i, rows[4 * i : 4 * i + 4], chosen)
        return chosen

    lds = []
    for o in range(4):
        s = slot_seq(o)
        w0, w1 = wst[:, :, 0:512].reshape(32, 512), wst[:, :, 512:1024].reshape(32, 512)
        all_raw = dot(w0, x_b[s, 0], ((1,), (1,))) + dot(w1, x_b[s, 1], ((1,), (1,)))
        raw = jnp.concatenate([pick(all_raw[0:16], f, 4), pick(all_raw[16:32], f, 4)], axis=0)
        odd = lax.rem(f, 2)
        extra = jnp.concatenate([pick(de[s, 0], odd, 2), pick(de[s, 1], odd, 2)], axis=0)
        stp = jnp.maximum(raw, 0.0) + jnp.log1p(jnp.exp(-jnp.abs(raw)))
        stp_s[o] = stp
        lds.append(extra - stp * rate)
    ld = jnp.concatenate(lds, axis=0)
    ld_a = ld.astype(BF16)
    rest = ld - ld_a.astype(F32)
    ld_b = rest.astype(BF16)
    ld_c = (rest - ld_b.astype(F32)).astype(BF16)
    ld3 = jnp.concatenate([ld_a, ld_b, ld_c], axis=0)
    pre = dot(ld3, (ii <= jj).astype(F32).astype(BF16))
    suf = dot(ld3, (ii >= jj).astype(F32).astype(BF16))
    pre = pre[0:32] + (pre[32:64] + pre[64:96])
    suf = suf[0:32] + (suf[32:64] + suf[64:96])
    fwd_row = lax.rem(lax.broadcasted_iota(jnp.int32, (32, T), 0), 8) < 4
    cum = jnp.where(fwd_row, pre, suf)
    cum_s[...] = cum.reshape(4, 8, T)
    lane4 = lax.broadcasted_iota(jnp.int32, (1, 256), 1) // 64
    ends = []
    for o in range(4):
        for r in range(2):
            row = jnp.zeros((1, 256), F32)
            for h in range(4):
                i = o * 8 + r * 4 + h
                e = cum[i : i + 1, T - 1 : T] if r == 0 else cum[i : i + 1, 0:1]
                row = jnp.where(lane4 == h, e, row)
            ends.append(row)
    dec[...] = jnp.concatenate(ends, axis=0)
    own_dec = local(dec, d1.at[y])
    sd1 = [send(dec, d1.at[y], {"y": ymod(d)}) for d in near_first]

    halo_local.wait()
    for c in halos:
        c.wait_recv()
    zr[3].wait_recv()
    yr[3].wait_recv()

    def rows_of(w, k, n):
        return w[4 * k : 4 * k + 4].reshape(512, n)

    h0 = hall[:, 0].reshape(128, 512)
    h1 = hall[:, 1].reshape(128, 512)
    side = lax.rem(lax.broadcasted_iota(jnp.int32, (128, 256), 0) // 16, 2)
    gone = jnp.logical_or(
        jnp.logical_and(side == 0, sp == 0), jnp.logical_and(side == 1, sp == 63)
    )
    for i, w in enumerate((wa1, wa2)):
        hproj = (dot(h0, rows_of(w, 0, 256)) + dot(h1, rows_of(w, 1, 256))).astype(BF16).astype(F32)
        hp[:, :, :, i * 256 : (i + 1) * 256] = jnp.where(gone, 0.0, hproj).reshape(4, 2, 16, 256)

    def spread(cols, c):
        parts = [
            jnp.where(low, cols[:, c + 2 * q : c + 2 * q + 1], cols[:, c + 2 * q + 1 : c + 2 * q + 2])
            for q in range(2)
        ]
        return jnp.concatenate(parts, axis=1)

    def front(o, hf):
        s = slot_seq(o)
        x0, x1 = x_b[s, 0], x_b[s, 1]
        for i, w in enumerate((wa1, wa2)):
            pa = dot(x0, rows_of(w, 0, 256)) + dot(x1, rows_of(w, 1, 256))
            p_s[16:272, i * 256 : (i + 1) * 256] = pa.astype(BF16).astype(F32)
        p_s[0:16, :] = hp[s, 0]
        p_s[272:288, :] = hp[s, 1]
        conv = p_s[14 : 14 + T, :] * par[0:1, :]
        for j in range(1, 5):
            conv = conv + p_s[14 + j : 14 + j + T, :] * par[j : j + 1, :]
        act = silu(conv)
        v, b, c = act[:, 0:256], act[:, 256:384], act[:, 384:512]
        cols = jnp.concatenate([cum_s[o], stp_s[o], jnp.zeros((112, T), F32)], axis=0).T
        cols_s[o] = cols
        v_s[o] = v.astype(BF16)
        b_s[o] = b.astype(BF16)
        c_s[o] = c.astype(BF16)
        bt = b.T.astype(BF16)
        lane = lax.broadcasted_iota(jnp.int32, (1, 128), 1)
        end = jnp.where(lane < 4, cols[T - 1 : T, :], cols[0:1, :])
        w_end = jnp.exp(end - cols)
        n = (o - 2 * hf) * 2
        for r in range(2):
            scale = spread(w_end, 4 * r) * spread(cols, 8 + 4 * r)
            st[hf, :, n + r] = dot(bt, (v * scale).astype(BF16)).astype(BF16).reshape(8, 16, 256)

    s1, own_st = [], []
    for hf in range(2):

        def front_step(o, _, hf=hf):
            front(o, hf)
            return _

        lax.fori_loop(2 * hf, 2 * hf + 2, front_step, 0)
        own_st.append(local(st.at[hf, y], r1.at[hf, y]))
        s1.append([send(st.at[hf, ymod(d)], r1.at[hf, y], {"y": ymod(d)}) for d in near_first])
        gate_step(hf + 1)
        if hf == 0:
            own_dec.wait()
            for c in sd1:
                c.wait_recv()
            cumf = jnp.zeros((8, 256), F32)
            cumb = jnp.zeros((8, 256), F32)
            back = lax.rem(lax.broadcasted_iota(jnp.int32, (8, 256), 0), 2) == 1
            pf = []
            for i in range(8):
                pf.append(cumf)
                cumf = cumf + d1[i]
            for i in reversed(range(8)):
                pd[i] = jnp.exp(jnp.where(back, cumb, pf[i]))
                cumb = cumb + d1[i]
            totd[...] = cumf
            own_td = local(totd, d2.at[z])
            sd2 = [send(totd, d2.at[z], {"z": zmod(d)}) for d in near_first]

    def inner(o, _):
        cols, cu, stp = cols_s[o], cum_s[o], stp_s[o]
        scores = dot(c_s[o], b_s[o], ((1,), (1,)))
        for q in range(2):
            vp = v_s[o, :, q * 128 : (q + 1) * 128]
            both = []
            for e in range(2):
                h = 2 * q + e
                expo = jnp.where(
                    jj <= ii,
                    cols[:, h : h + 1] - cu[h : h + 1, :],
                    cols[:, 4 + h : 5 + h] - cu[4 + h : 5 + h, :],
                )
                df, db = stp[h : h + 1, :], stp[4 + h : 5 + h, :]
                dts = jnp.where(jj < ii, df, jnp.where(jj > ii, db, df + db))
                both.append(dot((scores * jnp.exp(expo) * dts).astype(BF16), vp))
            y_s[o, :, q * 128 : (q + 1) * 128] = jnp.where(low, both[0], both[1])
        return _

    def scan1(hf):
        own_st[hf].wait()
        for c in s1[hf]:
            c.wait_recv()
        for n in range(4):
            run = jnp.zeros((16, 256), F32)
            for i in range(8) if n % 2 == 0 else reversed(range(8)):
                res[hf, i, n] = run
                w = jnp.exp(d1[i, 4 * hf + n : 4 * hf + n + 1, :])
                run = run * w + r1[hf, i, n].astype(F32)
            tot[hf, n] = run.astype(BF16)
        mine = local(tot.at[hf], r2.at[hf, z])
        return mine, [send(tot.at[hf], r2.at[hf, z], {"z": zmod(d)}) for d in near_first]

    def scan2(hf, s2):
        s2[0].wait()
        for c in s2[1]:
            c.wait_recv()
        for n in range(4):
            acc = jnp.zeros((16, 256), F32)
            for i in range(8) if n % 2 == 0 else reversed(range(8)):
                w = jnp.exp(d2[i, 4 * hf + n : 4 * hf + n + 1, :])
                new = acc * w + r2[hf, i, n].astype(F32)
                used = (i < z) if n % 2 == 0 else (i > z)
                acc = jnp.where(used, new, acc)
            for i in range(8):
                w = pd[i, 4 * hf + n : 4 * hf + n + 1, :]
                r1[hf, i, n] = (res[hf, i, n] + acc * w).astype(BF16)
        mine = local(r1.at[hf, y], inc.at[hf, y])
        return mine, [send(r1.at[hf, ymod(d)], inc.at[hf, y], {"y": ymod(d)}) for d in near_first]

    lax.fori_loop(0, 2, inner, 0)
    s2_0 = scan1(0)
    gate_step(3)

    gate_step(4)

    def gates(o, _):
        s = slot_seq(o)
        x0, x1 = x_b[s, 0], x_b[s, 1]
        g = dot(x0, rows_of(wb1, 0, 256)) + dot(x1, rows_of(wb1, 1, 256))
        gate[o] = silu(g.astype(BF16).astype(F32))
        q = dot(x0, rows_of(wb2, 0, 128)) + dot(x1, rows_of(wb2, 1, 128))
        pool[1, o] = q.astype(BF16)
        return _

    lax.fori_loop(0, 4, gates, 0)

    def pool_copies(g):
        n = GRID_W << g
        spans = ((T - n, 0, 0, nxt), (0, 2, 1, prv))
        return [
            pltpu.make_async_remote_copy(
                src_ref=pool.at[1, :, pl.ds(a, n)], dst_ref=pool.at[b, :, pl.ds(a, n)],
                send_sem=psem.at[0, i], recv_sem=psem.at[1, i], device_id=dev, device_id_type=MESH,
            )
            for a, b, i, dev in spans
        ]

    for g in range(4):

        @pl.when(group_at == g)
        def _():
            for c in pool_copies(g):
                c.start()

    s2_1 = scan1(1)
    own_td.wait()
    for c in sd2:
        c.wait_recv()
    s3_0 = scan2(0, s2_0)
    wos = []
    for d in (1, 3, 2):
        g = fmod(d)
        wos.append(send(woi_in.at[at(g, 256)], woi.at[f], {"fs": g}))
        wos.append(send(wop_in.at[at(g // 2, 256)], wop.at[f], {"fs": g}))
    lax.fori_loop(2, 4, inner, 0)
    s3_1 = scan2(1, s2_1)

    k = jnp.left_shift(jnp.int32(2), group_at)
    ti = lax.broadcasted_iota(jnp.int32, (T, 3 * T), 0)
    tj = lax.broadcasted_iota(jnp.int32, (T, 3 * T), 1)
    ri, ci_ = ti // GRID_W + 8, lax.rem(ti, GRID_W)
    rj, cj = tj // GRID_W, lax.rem(tj, GRID_W)
    grow = rj + (sp * 8 - 8)
    inside = (rj >= ri - k // 2) & (rj < ri + k // 2) & (cj >= ci_ - k // 2) & (cj < ci_ + k // 2)
    inside = inside & (grow >= 0) & (grow < 512)
    m_s[...] = inside.astype(F32).astype(BF16)
    for g in range(4):

        @pl.when(group_at == g)
        def _():
            for c in pool_copies(g):
                c.wait()
    row = lax.broadcasted_iota(jnp.int32, (T, 128), 0) // GRID_W + sp * 8
    col = lax.rem(lax.broadcasted_iota(jnp.int32, (T, 128), 0), GRID_W)
    cells = (
        (jnp.minimum(row + k // 2, 512) - jnp.maximum(row - k // 2, 0))
        * (jnp.minimum(col + k // 2, GRID_W) - jnp.maximum(col - k // 2, 0))
    ).astype(F32)
    pgain = jnp.concatenate([pg[pl.ds(2 * group_at + i, 1), :] for i in range(2)], axis=1)
    ngain = jnp.concatenate([ng[pl.ds(8 * t + 2 * f + i, 1), :] for i in range(2)], axis=1)

    def pools(o, _):
        rows = jnp.concatenate([pool[0, o], pool[1, o], pool[2, o]], axis=0)
        off = dot(m_s[...], rows) / cells - pool[1, o].astype(F32)
        pld_s[o] = (dot(off.astype(BF16), pmix[...]) * pgain).astype(BF16)
        return _

    lax.fori_loop(0, 4, pools, 0)

    for c in wos:
        c.wait_recv()
    blk = ((ii // 64 == jj // 64).astype(F32) * (1.0 / 64.0)).astype(BF16)

    def finish(o):
        hf, n = o // 2, (o % 2) * 2
        cb, cols = c_s[o], jnp.exp(cols_s[o])
        carried = dot(cb, inc[hf, :, n].reshape(128, 256)) * spread(cols, 0)
        carried = carried + dot(cb, inc[hf, :, n + 1].reshape(128, 256)) * spread(cols, 4)
        g = (y_s[o] + carried) * gate[o]
        ms = dot((g * g).astype(BF16), blk)
        mix_s[...] = (g * lax.rsqrt(ms + EPSILON) * ngain).astype(BF16)

    mine = at(t, 128)
    theirs = at(1 - t, 128)
    far = []
    for o in range(4):
        if o % 2 == 0:
            s3 = s3_0 if o == 0 else s3_1
            s3[0].wait()
            for c in s3[1]:
                c.wait_recv()
        finish(o)
        for q in range(4):
            cs = slice(q * 256, (q + 1) * 256)
            part = dot(mix_s[theirs, :], woi[q]) + dot(pld_s[o, theirs, :], wop[q])
            dsend[o, :, cs] = part.astype(BF16)
        swap = send(dsend.at[o], drecv.at[o], pair)
        for q in range(4):
            cs = slice(q * 256, (q + 1) * 256)
            own[o, :, cs] = dot(mix_s[mine, :], woi[q]) + dot(pld_s[o, mine, :], wop[q])
        swap.wait_recv()
        chip = own[o] + drecv[o].astype(F32)
        if o == 0:
            raws[...] = chip.astype(BF16).reshape(2, 64, 1024)
            up = send(raws.at[0], rawr.at[0], {"fs": fmod(1)})
            down = send(raws.at[1], rawr.at[1], {"fs": fmod(3)})
        elif o == 1:
            up.wait_recv()
            xsend[0, 0:64] = (chip[0:64] + rawr[0].astype(F32)).astype(BF16)
            xsend[0, 64:128] = chip[64:128].astype(BF16)
            far.append(send(xsend.at[0], xrecv.at[0], {"fs": fmod(1)}))
        elif o == 2:
            down.wait_recv()
            xsend[1, 0:64] = chip[0:64].astype(BF16)
            xsend[1, 64:128] = (chip[64:128] + rawr[1].astype(F32)).astype(BF16)
            far.append(send(xsend.at[1], xrecv.at[1], {"fs": fmod(3)}))
        else:
            own[o] = chip
    for c in far:
        c.wait_recv()
    out[0] = (own[3] + xrecv[0].astype(F32) + xrecv[1].astype(F32)).astype(BF16)
    for c in sent:
        c.wait_send()


N_REMOTE = 150


def body(
    tokens, w_inner, w_gate, w_write, w_read, w_pool_in, w_step, conv_inner, conv_cross, rate_log,
    decay_extra, norm_gain, pool_mix, pool_gain, w_out_inner, w_out_pool,
):
    hbm = pl.BlockSpec(memory_space=pl.ANY)
    V = pltpu.VMEM
    scratch = [
        V((4, 2, T, 512), BF16),
        V((2, 16, 512), BF16),
        V((4, 2, 2, 16, 512), BF16),
        V((8, 8, 16, 256), BF16),
        V((8, 8, 16, 256), BF16),
        V((8, 8, 16, 256), BF16),
        V((8, 8, 16, 128), BF16),
        V((4, 256, 256), BF16),
        V((4, 256, 256), BF16),
        V((4, 2, 8, T), F32),
        V((128, 256), BF16),
        V((2, 16, 1024), BF16),
        V((5, 256), BF16),
        V((5, 2, 128), BF16),
        V((16, 128), F32),
        V((8, 128), F32),
        V((8, 512), F32),
        V((288, 512), F32),
        V((4, 2, 16, 512), F32),
        V((4, T, 256), F32),
        V((4, T, 256), BF16),
        V((4, T, 128), BF16),
        V((4, T, 128), BF16),
        V((4, 8, T), F32),
        V((4, 8, T), F32),
        V((4, T, 128), F32),
        V((4, T, 256), F32),
        V((3, 4, T, 128), BF16),
        V((T, 3 * T), BF16),
        V((2, 8, 4, 16, 256), BF16),
        V((8, 256), F32),
        V((2, 8, 4, 16, 256), BF16),
        V((8, 8, 256), F32),
        V((8, 8, 256), F32),
        V((2, 8, 4, 16, 256), BF16),
        V((8, 8, 256), F32),
        V((8, 256), F32),
        V((2, 8, 4, 16, 256), F32),
        V((2, 4, 16, 256), BF16),
        V((2, 8, 4, 16, 256), BF16),
        V((4, 128, 1024), F32),
        V((4, 128, 1024), BF16),
        V((4, 128, 1024), BF16),
        V((2, 64, 1024), BF16),
        V((2, 64, 1024), BF16),
        V((2, 128, 1024), BF16),
        V((2, 128, 1024), BF16),
        V((T, 256), BF16),
        V((4, T, 256), BF16),
        pltpu.SemaphoreType.DMA((32,)),
        pltpu.SemaphoreType.DMA((N_REMOTE,)),
        pltpu.SemaphoreType.DMA((N_REMOTE,)),
        pltpu.SemaphoreType.DMA((2, 2)),
    ]
    return pl.pallas_call(
        kernel,
        out_shape=jax.ShapeDtypeStruct((1, 128, 1024), BF16),
        in_specs=[hbm] * 9 + [pl.BlockSpec(memory_space=pltpu.SMEM)] + [hbm] * 6,
        out_specs=pl.BlockSpec(memory_space=pltpu.VMEM),
        scratch_shapes=scratch,
        compiler_params=pltpu.CompilerParams(
            collective_id=0, has_side_effects=True, vmem_limit_bytes=60 * 1024 * 1024
        ),
    )(
        tokens, w_inner, w_gate, w_write, w_read, w_pool_in, jnp.transpose(w_step, (1, 2, 0)),
        conv_inner, conv_cross, rate_log, jnp.transpose(decay_extra[0], (1, 2, 0)),
        norm_gain.reshape(16, 128), pool_mix, pool_gain.reshape(8, 128), w_out_inner, w_out_pool,
    )


def solution(mesh):
    finer = Mesh(
        mesh.devices.reshape(8, 8, mesh.shape["fs"], mesh.shape["tp"]), ("z", "y", "fs", "tp")
    )
    in_specs = (
        P("fs", SP, "tp"),
        P(SP, "tp"),
        P(SP, "tp"),
        P(SP, "tp"),
        P(SP, "tp"),
        P(SP, "tp"),
        P(),
        P(),
        P(),
        P(),
        P("fs", SP, None, "tp"),
        P(),
        P(),
        P(),
        P("tp", "fs"),
        P("tp", "fs"),
    )
    out_specs = P("fs", ("z", "y", "tp"), None)
    return jax.shard_map(body, mesh=finer, in_specs=in_specs, out_specs=out_specs, check_vma=False)
```

```python
import functools

import jax
import jax.numpy as jnp
from jax import lax
from jax.experimental import pallas as pl
from jax.experimental.pallas import tpu as pltpu
from jax.sharding import Mesh
from jax.sharding import PartitionSpec as P

MESH = pl.DeviceIdType.MESH
F32, BF16 = jnp.float32, jnp.bfloat16
SP = ("z", "y")
EPSILON = 1e-05
T = 256
GRID_W = 32


def silu(v):
    return (0.5 * v) * (1.0 + jnp.tanh(0.5 * v))


def dot(a, b, dims=((1,), (0,)), **kw):
    return lax.dot_general(a, b, (dims, ((), ())), preferred_element_type=F32, **kw)


def kernel(
    tok, w_inner, w_gate, w_write, w_read, w_pool, wst_in, ci_in, cc_in, rate_in, dec_in, ng_in, pmix_in,
    pg_in, woi_in, wop_in,
    out,
    x_b, hrow, hall, wa1, wa2, wb1, wb2, alt1, alt3, alt4, woi, wop, de, pmix, wst, ci, cc, ng, pg, par,
    p_s, hp, y_s, v_s, b_s, c_s, cum_s, stp_s, cols_s, gate, pool, m_s,
    sb, dec, decp, st, r1, d1, pd, r2, d2, totd, res, tot, inc, b_in, own, dsend, drecv, raws, rawr, xsend, xrecv,
    mix_s, pld_s,
    lsem, ssem, rsem, psem,
):
    z, y, f, t = (lax.axis_index(a) for a in ("z", "y", "fs", "tp"))
    fq, yq, yp = lax.rem(f, 2), lax.rem(y, 2), y // 2
    r = fq * 2 + yq
    sp = z * 8 + y
    group_at = t * 2 + fq

    def along(d):
        v = lax.rem(sp + d, 64)
        return {"z": v // 8, "y": lax.rem(v, 8)}

    count = [0, 0]
    sent = []

    def send(src, dst, dev):
        i = count[0]
        count[0] += 1
        c = pltpu.make_async_remote_copy(
            src_ref=src, dst_ref=dst, send_sem=ssem.at[i], recv_sem=rsem.at[i],
            device_id=dev, device_id_type=MESH,
        )
        c.start()
        sent.append(c)
        return c

    def local(src, dst):
        c = pltpu.make_async_copy(src, dst, lsem.at[count[1]])
        count[1] += 1
        c.start()
        return c

    def ymod(d):
        return lax.rem(y + d, 8)

    def zmod(d):
        return lax.rem(z + d, 8)

    def fmod(d):
        return lax.rem(f + d, 4)

    def pmod(d):
        return lax.rem(yp + d, 4)

    f_flip, y_flip = f + 1 - 2 * fq, y + 1 - 2 * yq
    r_x, r_y, r_d = (1 - fq) * 2 + yq, fq * 2 + 1 - yq, 3 - r
    to_x, to_y, to_d = {"fs": f_flip}, {"y": y_flip}, {"fs": f_flip, "y": y_flip}

    def at(v, n):
        return pl.ds(pl.multiple_of(v * n, n), n)

    near_first = (1, 7, 2, 6, 3, 5, 4)
    pair = {"tp": 1 - t}
    group = [pair] + [{**a, "tp": e} for a in (to_x, to_y, to_d) for e in (t, 1 - t)]
    peers = [{"y": ymod(d)} for d in range(1, 8)] + [{"z": zmod(d)} for d in range(1, 8)]
    peers += group + [{"fs": fmod(d)} for d in range(1, 4)] + [along(d) for d in (1, 63, 2, 62)]

    pool[:, 0] = jnp.zeros((2, T, 128), BF16)
    pool[:, 3] = jnp.zeros((2, T, 128), BF16)
    barrier = pltpu.get_barrier_semaphore()
    for p in peers:
        pl.semaphore_signal(barrier, inc=1, device_id=p, device_id_type=MESH)
    mine1, mine2, mine3, mine4 = (w.at[z, y] for w in (wa1, wa2, wb1, wb2))
    tok_local = local(tok.at[0], x_b.at[r, t])
    w_local = [
        local(w_inner.at[:, at(r, 256)], mine1),
        local(w_inner.at[:, at(r_y, 256)], alt1),
        local(w_write.at[:, at(fq, 128)], mine2.at[:, pl.ds(0, 128)]),
        local(w_read.at[:, at(fq, 128)], mine2.at[:, pl.ds(128, 128)]),
        local(w_gate.at[:, at(r, 256)], mine3),
        local(w_gate.at[:, at(r_y, 256)], alt3),
        local(w_pool.at[:, at(r, 128)], mine4),
        local(w_pool.at[:, at(r_y, 128)], alt4),
    ]
    others = [
        local(wst_in.at[:, at(t, 16)], wst),
        local(dec_in.at[:, at(fq, 8)], de.at[r]),
        local(ci_in.at[:, at(t * 4 + r, 256)], ci),
        local(cc_in.at[:, :, at(group_at, 128)], cc),
        local(ng_in, ng),
        local(pg_in, pg),
        local(pmix_in.at[group_at, at(yq, 128)], pmix),
        local(woi_in.at[at(r, 256)], woi.at[f]),
        local(wop_in.at[at(fq, 256)], wop.at[f]),
    ]
    tok_local.wait()
    for c in w_local:
        c.wait()
    pl.semaphore_wait(barrier, len(peers))

    x_own = x_b.at[r, t]
    edge_n = send(x_own.at[pl.ds(240, 16)], hrow.at[0], along(1))
    edge_p = send(x_own.at[pl.ds(0, 16)], hrow.at[1], along(63))

    def stage(mine, alt):
        return [send(alt if d % 2 else mine, mine, {"y": ymod(d)}) for d in near_first]

    first, second = stage(mine1, alt1), stage(mine2, mine2)
    x_right = send(x_own, x_own, to_x)
    x_left = send(x_own, x_own, to_y)
    x_pair = [send(x_own, x_own, pair)]
    decs = [
        send(dec_in.at[:, at(q, 8)], de.at[r], g)
        for q, g in ((1 - fq, to_x), (fq, to_y), (1 - fq, to_d))
    ]
    third, fourth = stage(mine3, alt3), stage(mine4, alt4)

    def ring_z(w, k, to):
        s = w.at[zmod(8 - k if to == 1 else k)]
        if k == 3:
            s = s.at[pl.ds(0 if to == 1 else 4, 4)]
        return send(s, s, {"z": zmod(to)})

    rings = {}

    def begin(name, w):
        rings[name] = [(w, to, [ring_z(w, 0, to)]) for to in (1, 7)]

    def step(names, k):
        for name in names:
            for w, to, ring in rings[name]:
                ring[k - 1].wait_recv()
                if k < 4:
                    ring.append(ring_z(w, k, to))

    for c in first:
        c.wait_recv()
    begin("a1", wa1)
    for c in second:
        c.wait_recv()
    begin("a2", wa2)
    edge_n.wait_recv()
    edge_p.wait_recv()
    halo_local = local(hrow, hall.at[r, t])
    halos = [send(hrow, hall.at[r, t], g) for g in group]
    step(("a1", "a2"), 1)
    x_right.wait_recv()
    block = x_b.at[r_x, t]
    x_fr = send(block.at[pl.ds(0, 128)], block.at[pl.ds(0, 128)], to_y)
    x_pair.append(send(block, block, pair))
    x_left.wait_recv()
    block = x_b.at[r_y, t]
    x_fl = send(block.at[pl.ds(128, 128)], block.at[pl.ds(128, 128)], to_x)
    x_pair.append(send(block, block, pair))
    step(("a1", "a2"), 2)
    for c in others:
        c.wait()
    par[0:5, 0:256] = ci[...].astype(F32)
    par[0:5, 256:384] = cc[:, 0, :].astype(F32)
    par[0:5, 384:512] = cc[:, 1, :].astype(F32)
    x_fr.wait_recv()
    x_fl.wait_recv()
    block = x_b.at[r_d, t]
    x_pair.append(send(block, block, pair))
    step(("a1", "a2"), 3)
    for c in third + fourth:
        c.wait_recv()
    begin("b1", wb1)
    begin("b2", wb2)
    wos = []
    for d in (1, 3, 2):
        g = fmod(d)
        q = lax.rem(g, 2)
        wos.append(send(woi_in.at[at(q * 2 + yq, 256)], woi.at[f], {"fs": g}))
        wos.append(send(wop_in.at[at(q, 256)], wop.at[f], {"fs": g}))

    def gate_step(k):
        step(("b1", "b2"), k)

    for c in x_pair + decs:
        c.wait_recv()
    ii = lax.broadcasted_iota(jnp.int32, (T, T), 0)
    jj = lax.broadcasted_iota(jnp.int32, (T, T), 1)
    low = lax.broadcasted_iota(jnp.int32, (T, 128), 1) < 64

    def slot_block(o):
        return lax.rem(yq + lax.rem(3 - o, 2), 2)

    def slot_unit(o):
        return lax.rem(fq + (3 - o) // 2, 2) * 2 + slot_block(o)

    r8 = lax.broadcasted_iota(jnp.int32, (8, 1), 0)
    rate = jnp.zeros((8, 1), F32)
    for i in range(8):
        rate = jnp.where(r8 == i, rate_in[i // 4, t * 16 + r * 4 + i % 4], rate)
    rate = jnp.exp(rate)
    def pick(rows, which, n):
        chosen = rows[0:4]
        for i in range(1, n):
            chosen = jnp.where(which == i, rows[4 * i : 4 * i + 4], chosen)
        return chosen

    lds = []
    for o in range(4):
        s = slot_unit(o)
        w0, w1 = wst[:, :, 0:512].reshape(32, 512), wst[:, :, 512:1024].reshape(32, 512)
        all_raw = dot(w0, x_b[s, 0], ((1,), (1,))) + dot(w1, x_b[s, 1], ((1,), (1,)))
        raw = jnp.concatenate([pick(all_raw[0:16], r, 4), pick(all_raw[16:32], r, 4)], axis=0)
        extra = jnp.concatenate([pick(de[s, 0], yq, 2), pick(de[s, 1], yq, 2)], axis=0)
        stp = jnp.maximum(raw, 0.0) + jnp.log1p(jnp.exp(-jnp.abs(raw)))
        stp_s[o] = stp
        lds.append(extra - stp * rate)
    ld = jnp.concatenate(lds, axis=0)
    ld_a = ld.astype(BF16)
    rest = ld - ld_a.astype(F32)
    ld_b = rest.astype(BF16)
    ld_c = (rest - ld_b.astype(F32)).astype(BF16)
    ld3 = jnp.concatenate([ld_a, ld_b, ld_c], axis=0)
    pre = dot(ld3, (ii <= jj).astype(F32).astype(BF16))
    suf = dot(ld3, (ii >= jj).astype(F32).astype(BF16))
    pre = pre[0:32] + (pre[32:64] + pre[64:96])
    suf = suf[0:32] + (suf[32:64] + suf[64:96])
    fwd_row = lax.rem(lax.broadcasted_iota(jnp.int32, (32, T), 0), 8) < 4
    cum = jnp.where(fwd_row, pre, suf)
    cum_s[...] = cum.reshape(4, 8, T)
    lane4 = lax.broadcasted_iota(jnp.int32, (1, 256), 1) // 64
    ends = []
    for o in range(4):
        for n in range(2):
            row = jnp.zeros((1, 256), F32)
            for h in range(4):
                i = o * 8 + n * 4 + h
                e = cum[i : i + 1, T - 1 : T] if n == 0 else cum[i : i + 1, 0:1]
                row = jnp.where(lane4 == h, e, row)
            ends.append(row)
    dec[...] = jnp.concatenate(ends, axis=0)
    both = [ends[4 * hf + n] + ends[4 * hf + 2 + n] for hf in range(2) for n in range(2)]
    decp[...] = jnp.concatenate(both + [jnp.zeros((4, 256), F32)], axis=0)
    own_dec = local(decp, d1.at[yp])
    sd1 = [send(decp, d1.at[yp], {"y": ymod(2 * d)}) for d in (1, 3, 2)]

    halo_local.wait()
    for c in halos:
        c.wait_recv()
    step(("a1", "a2"), 4)

    def rows_of(w, k, n):
        return w[4 * k : 4 * k + 4].reshape(512, n)

    h0 = hall[:, 0].reshape(128, 512)
    h1 = hall[:, 1].reshape(128, 512)
    hrow_at = lax.broadcasted_iota(jnp.int32, (128, 256), 0)
    side = lax.rem(hrow_at // 16, 2)
    place = sp - yq + lax.rem(hrow_at // 32, 2)
    gone = jnp.logical_or(
        jnp.logical_and(side == 0, place == 0), jnp.logical_and(side == 1, place == 63)
    )
    for i, w in enumerate((wa1, wa2)):
        hproj = (dot(h0, rows_of(w, 0, 256)) + dot(h1, rows_of(w, 1, 256))).astype(BF16).astype(F32)
        hp[:, :, :, i * 256 : (i + 1) * 256] = jnp.where(gone, 0.0, hproj).reshape(4, 2, 16, 256)

    def spread(cols, c):
        parts = [
            jnp.where(low, cols[:, c + 2 * q : c + 2 * q + 1], cols[:, c + 2 * q + 1 : c + 2 * q + 2])
            for q in range(2)
        ]
        return jnp.concatenate(parts, axis=1)

    def front(o):
        s = slot_unit(o)
        x0, x1 = x_b[s, 0], x_b[s, 1]
        for i, w in enumerate((wa1, wa2)):
            pa = dot(x0, rows_of(w, 0, 256)) + dot(x1, rows_of(w, 1, 256))
            p_s[16:272, i * 256 : (i + 1) * 256] = pa.astype(BF16).astype(F32)
        p_s[0:16, :] = hp[s, 0]
        p_s[272:288, :] = hp[s, 1]
        conv = p_s[14 : 14 + T, :] * par[0:1, :]
        for j in range(1, 5):
            conv = conv + p_s[14 + j : 14 + j + T, :] * par[j : j + 1, :]
        act = silu(conv)
        v, b, c = act[:, 0:256], act[:, 256:384], act[:, 384:512]
        cols = jnp.concatenate([cum_s[o], stp_s[o], jnp.zeros((112, T), F32)], axis=0).T
        cols_s[o] = cols
        v_s[o] = v.astype(BF16)
        b_s[o] = b.astype(BF16)
        c_s[o] = c.astype(BF16)
        bt = b.T.astype(BF16)
        lane = lax.broadcasted_iota(jnp.int32, (1, 128), 1)
        end = jnp.where(lane < 4, cols[T - 1 : T, :], cols[0:1, :])
        w_end = jnp.exp(end - cols)
        for n in range(2):
            scale = spread(w_end, 4 * n) * spread(cols, 8 + 4 * n)
            sb[o, n] = dot(bt, (v * scale).astype(BF16))

    def early_late(hf):
        return 2 * hf + 1 - yq, 2 * hf + yq

    def fade(o, n):
        return jnp.exp(dec[pl.ds(2 * o + n, 1), :])

    def join(hf):
        e, l = early_late(hf)
        ahead = sb[e, 0] * fade(l, 0) + sb[l, 0]
        behind = sb[l, 1] * fade(e, 1) + sb[e, 1]
        st[hf, :, 0] = ahead.astype(BF16).reshape(4, 32, 256)
        st[hf, :, 1] = behind.astype(BF16).reshape(4, 32, 256)

    def enter(hf):
        e, l = early_late(hf)
        ahead = inc[hf, :, 0].reshape(128, 256)
        behind = inc[hf, :, 1].reshape(128, 256)
        b_in[e, 0] = ahead
        b_in[l, 0] = (ahead.astype(F32) * fade(e, 0) + sb[e, 0]).astype(BF16)
        b_in[l, 1] = behind
        b_in[e, 1] = (behind.astype(F32) * fade(l, 1) + sb[l, 1]).astype(BF16)

    s1, own_st = [], []
    for hf in range(2):

        def front_step(o, _):
            front(o)
            return _

        lax.fori_loop(2 * hf, 2 * hf + 2, front_step, 0)
        join(hf)
        own_st.append(local(st.at[hf, yp], r1.at[hf, yp]))
        s1.append([send(st.at[hf, pmod(d)], r1.at[hf, yp], {"y": ymod(2 * d)}) for d in (1, 3, 2)])
        gate_step(hf + 1)
        if hf == 0:
            own_dec.wait()
            for c in sd1:
                c.wait_recv()
            cumf = jnp.zeros((8, 256), F32)
            cumb = jnp.zeros((8, 256), F32)
            back = lax.rem(lax.broadcasted_iota(jnp.int32, (8, 256), 0), 2) == 1
            pf = []
            for i in range(4):
                pf.append(cumf)
                cumf = cumf + d1[i]
            for i in reversed(range(4)):
                pd[i] = jnp.exp(jnp.where(back, cumb, pf[i]))
                cumb = cumb + d1[i]
            totd[...] = cumf
            sd2 = [send(totd, d2.at[z], {"z": zmod(d)}) for d in near_first]

    def inner(o, _):
        cols, cu, stp = cols_s[o], cum_s[o], stp_s[o]
        scores = dot(c_s[o], b_s[o], ((1,), (1,)))
        for q in range(2):
            vp = v_s[o, :, q * 128 : (q + 1) * 128]
            both = []
            for e in range(2):
                h = 2 * q + e
                expo = jnp.where(
                    jj <= ii,
                    cols[:, h : h + 1] - cu[h : h + 1, :],
                    cols[:, 4 + h : 5 + h] - cu[4 + h : 5 + h, :],
                )
                df, db = stp[h : h + 1, :], stp[4 + h : 5 + h, :]
                dts = jnp.where(jj < ii, df, jnp.where(jj > ii, db, df + db))
                both.append(dot((scores * jnp.exp(expo) * dts).astype(BF16), vp))
            y_s[o, :, q * 128 : (q + 1) * 128] = jnp.where(low, both[0], both[1])
        return _

    def scan1(hf):
        own_st[hf].wait()
        for c in s1[hf]:
            c.wait_recv()
        for n in range(2):
            run = jnp.zeros((32, 256), F32)
            for i in range(4) if n == 0 else reversed(range(4)):
                res[hf, i, n] = run
                w = jnp.exp(d1[i, 2 * hf + n : 2 * hf + n + 1, :])
                run = run * w + r1[hf, i, n].astype(F32)
            tot[hf, n] = run.astype(BF16)
        return [
            send(tot.at[hf, (z + d) // 8], r2.at[hf, z, (z + d) // 8], {"z": zmod(d)})
            for d in near_first
        ]

    def scan2(hf, s2):
        for c in s2:
            c.wait_recv()
        for n in range(2):
            acc = jnp.zeros((32, 256), F32)
            for i in range(8) if n == 0 else reversed(range(8)):
                w = jnp.exp(d2[i, 2 * hf + n : 2 * hf + n + 1, :])
                new = acc * w + r2[hf, i, n].astype(F32)
                used = (i < z) if n == 0 else (i > z)
                acc = jnp.where(used, new, acc)
            for i in range(4):
                w = pd[i, 2 * hf + n : 2 * hf + n + 1, :]
                r1[hf, i, n] = (res[hf, i, n] + acc * w).astype(BF16)
        mine = local(r1.at[hf, yp], inc.at[hf, yp])
        return mine, [
            send(r1.at[hf, pmod(d)], inc.at[hf, yp], {"y": ymod(2 * d)}) for d in (1, 3, 2)
        ]

    def gates(o, _):
        s = slot_unit(o)
        x0, x1 = x_b[s, 0], x_b[s, 1]
        g = dot(x0, rows_of(wb1, 0, 256)) + dot(x1, rows_of(wb1, 1, 256))
        gate[o] = silu(g.astype(BF16).astype(F32))
        q = dot(x0, rows_of(wb2, 0, 128)) + dot(x1, rows_of(wb2, 1, 128))
        pool[o // 2, 1 + slot_block(o)] = q.astype(BF16)
        return _

    def pool_copies(g):
        n = GRID_W << g
        spans = ((2, 0, T - n, along(2)), (1, 3, 0, along(62)))
        return [
            pltpu.make_async_remote_copy(
                src_ref=pool.at[:, a, pl.ds(c, n)], dst_ref=pool.at[:, b, pl.ds(c, n)],
                send_sem=psem.at[0, i], recv_sem=psem.at[1, i], device_id=dev, device_id_type=MESH,
            )
            for i, (a, b, c, dev) in enumerate(spans)
        ]

    lax.fori_loop(0, 2, inner, 0)
    gate_step(3)
    s2_0 = scan1(0)
    lax.fori_loop(2, 4, inner, 0)
    gate_step(4)
    s2_1 = scan1(1)
    for c in sd2:
        c.wait_recv()
    s3_0 = scan2(0, s2_0)
    lax.fori_loop(0, 4, gates, 0)
    for g in range(4):

        @pl.when(group_at == g)
        def _():
            for c in pool_copies(g):
                c.start()

    s3_1 = scan2(1, s2_1)

    k = jnp.left_shift(jnp.int32(2), group_at)
    ti = lax.broadcasted_iota(jnp.int32, (T, 3 * T), 0)
    tj = lax.broadcasted_iota(jnp.int32, (T, 3 * T), 1)
    ri, ci_ = ti // GRID_W + 8, lax.rem(ti, GRID_W)
    rj, cj = tj // GRID_W, lax.rem(tj, GRID_W)
    inside = (rj >= ri - k // 2) & (rj < ri + k // 2) & (cj >= ci_ - k // 2) & (cj < ci_ + k // 2)
    m_s[...] = inside.astype(F32).astype(BF16)
    for g in range(4):

        @pl.when(group_at == g)
        def _():
            for c in pool_copies(g):
                c.wait()
    pool[:, 0] = jnp.where(sp // 2 == 0, jnp.zeros((2, T, 128), BF16), pool[:, 0])
    pool[:, 3] = jnp.where(sp // 2 == 31, jnp.zeros((2, T, 128), BF16), pool[:, 3])
    col = lax.rem(lax.broadcasted_iota(jnp.int32, (T, 128), 0), GRID_W)
    cols_in = jnp.minimum(col + k // 2, GRID_W) - jnp.maximum(col - k // 2, 0)
    pgain = jnp.concatenate([pg[pl.ds(2 * group_at + i, 1), :] for i in range(2)], axis=1)
    ngain = jnp.concatenate([ng[pl.ds(8 * t + 2 * r + i, 1), :] for i in range(2)], axis=1)

    def pools(o, _):
        b = slot_block(o)
        row = lax.broadcasted_iota(jnp.int32, (T, 128), 0) // GRID_W + (sp - yq + b) * 8
        cells = (jnp.minimum(row + k // 2, 512) - jnp.maximum(row - k // 2, 0)) * cols_in
        rows = jnp.concatenate([pool[o // 2, b + i] for i in range(3)], axis=0)
        off = dot(m_s[...], rows) / cells.astype(F32) - pool[o // 2, b + 1].astype(F32)
        pld_s[o] = (dot(off.astype(BF16), pmix[...]) * pgain).astype(BF16)
        return _

    lax.fori_loop(0, 4, pools, 0)

    for c in wos:
        c.wait_recv()
    blk = ((ii // 64 == jj // 64).astype(F32) * (1.0 / 64.0)).astype(BF16)

    def finish(o):
        cb, cols = c_s[o], jnp.exp(cols_s[o])
        carried = dot(cb, b_in[o, 0]) * spread(cols, 0) + dot(cb, b_in[o, 1]) * spread(cols, 4)
        g = (y_s[o] + carried) * gate[o]
        ms = dot((g * g).astype(BF16), blk)
        mix_s[...] = (g * lax.rsqrt(ms + EPSILON) * ngain).astype(BF16)

    mine = at(t, 128)
    theirs = at(1 - t, 128)
    far = []
    for o in range(4):
        if o % 2 == 0:
            s3 = s3_0 if o == 0 else s3_1
            s3[0].wait()
            for c in s3[1]:
                c.wait_recv()
            enter(o // 2)
        finish(o)
        for q in range(4):
            cs = slice(q * 256, (q + 1) * 256)
            part = dot(mix_s[theirs, :], woi[q]) + dot(pld_s[o, theirs, :], wop[q])
            dsend[o, :, cs] = part.astype(BF16)
        swap = send(dsend.at[o], drecv.at[o], pair)
        for q in range(4):
            cs = slice(q * 256, (q + 1) * 256)
            own[o, :, cs] = dot(mix_s[mine, :], woi[q]) + dot(pld_s[o, mine, :], wop[q])
        swap.wait_recv()
        chip = own[o] + drecv[o].astype(F32)
        if o == 0:
            raws[...] = chip.astype(BF16).reshape(2, 64, 1024)
            up = send(raws.at[0], rawr.at[0], to_x)
            down = send(raws.at[1], rawr.at[1], to_y)
        elif o == 1:
            down.wait_recv()
            xsend[0, 0:64] = chip[0:64].astype(BF16)
            xsend[0, 64:128] = (chip[64:128] + rawr[1].astype(F32)).astype(BF16)
            far.append(send(xsend.at[0], xrecv.at[0], to_x))
        elif o == 2:
            up.wait_recv()
            xsend[1, 0:64] = (chip[0:64] + rawr[0].astype(F32)).astype(BF16)
            xsend[1, 64:128] = chip[64:128].astype(BF16)
            far.append(send(xsend.at[1], xrecv.at[1], to_y))
        else:
            own[o] = chip
    for c in far:
        c.wait_recv()
    out[0] = (own[3] + xrecv[0].astype(F32) + xrecv[1].astype(F32)).astype(BF16)
    for c in sent:
        c.wait_send()


N_REMOTE = 150


def body(
    tokens, w_inner, w_gate, w_write, w_read, w_pool_in, w_step, conv_inner, conv_cross, rate_log,
    decay_extra, norm_gain, pool_mix, pool_gain, w_out_inner, w_out_pool,
):
    hbm = pl.BlockSpec(memory_space=pl.ANY)
    V = pltpu.VMEM
    scratch = [
        V((4, 2, T, 512), BF16),
        V((2, 16, 512), BF16),
        V((4, 2, 2, 16, 512), BF16),
        V((8, 8, 16, 256), BF16),
        V((8, 8, 16, 256), BF16),
        V((8, 8, 16, 256), BF16),
        V((8, 8, 16, 128), BF16),
        V((16, 256), BF16),
        V((16, 256), BF16),
        V((16, 128), BF16),
        V((4, 256, 256), BF16),
        V((4, 256, 256), BF16),
        V((4, 2, 8, T), F32),
        V((128, 256), BF16),
        V((2, 16, 1024), BF16),
        V((5, 256), BF16),
        V((5, 2, 128), BF16),
        V((16, 128), F32),
        V((8, 128), F32),
        V((8, 512), F32),
        V((288, 512), F32),
        V((4, 2, 16, 512), F32),
        V((4, T, 256), F32),
        V((4, T, 256), BF16),
        V((4, T, 128), BF16),
        V((4, T, 128), BF16),
        V((4, 8, T), F32),
        V((4, 8, T), F32),
        V((4, T, 128), F32),
        V((4, T, 256), F32),
        V((2, 4, T, 128), BF16),
        V((T, 3 * T), BF16),
        V((4, 2, 128, 256), F32),
        V((8, 256), F32),
        V((8, 256), F32),
        V((2, 4, 2, 32, 256), BF16),
        V((2, 4, 2, 32, 256), BF16),
        V((4, 8, 256), F32),
        V((4, 8, 256), F32),
        V((2, 8, 2, 32, 256), BF16),
        V((8, 8, 256), F32),
        V((8, 256), F32),
        V((2, 4, 2, 32, 256), F32),
        V((2, 2, 32, 256), BF16),
        V((2, 4, 2, 32, 256), BF16),
        V((4, 2, 128, 256), BF16),
        V((4, 128, 1024), F32),
        V((4, 128, 1024), BF16),
        V((4, 128, 1024), BF16),
        V((2, 64, 1024), BF16),
        V((2, 64, 1024), BF16),
        V((2, 128, 1024), BF16),
        V((2, 128, 1024), BF16),
        V((T, 256), BF16),
        V((4, T, 256), BF16),
        pltpu.SemaphoreType.DMA((32,)),
        pltpu.SemaphoreType.DMA((N_REMOTE,)),
        pltpu.SemaphoreType.DMA((N_REMOTE,)),
        pltpu.SemaphoreType.DMA((2, 2)),
    ]
    return pl.pallas_call(
        kernel,
        out_shape=jax.ShapeDtypeStruct((1, 128, 1024), BF16),
        in_specs=[hbm] * 9 + [pl.BlockSpec(memory_space=pltpu.SMEM)] + [hbm] * 6,
        out_specs=pl.BlockSpec(memory_space=pltpu.VMEM),
        scratch_shapes=scratch,
        compiler_params=pltpu.CompilerParams(
            collective_id=0, has_side_effects=True, vmem_limit_bytes=60 * 1024 * 1024
        ),
    )(
        tokens, w_inner, w_gate, w_write, w_read, w_pool_in, jnp.transpose(w_step, (1, 2, 0)),
        conv_inner, conv_cross, rate_log, jnp.transpose(decay_extra[0], (1, 2, 0)),
        norm_gain.reshape(16, 128), pool_mix, pool_gain.reshape(8, 128), w_out_inner, w_out_pool,
    )


def solution(mesh):
    finer = Mesh(
        mesh.devices.reshape(8, 8, mesh.shape["fs"], mesh.shape["tp"]), ("z", "y", "fs", "tp")
    )
    in_specs = (
        P("fs", SP, "tp"),
        P(SP, "tp"),
        P(SP, "tp"),
        P(SP, "tp"),
        P(SP, "tp"),
        P(SP, "tp"),
        P(),
        P(),
        P(),
        P(),
        P("fs", SP, None, "tp"),
        P(),
        P(),
        P(),
        P("tp", "fs"),
        P("tp", "fs"),
    )
    out_specs = P("fs", ("z", "y", "tp"), None)
    return jax.shard_map(body, mesh=finer, in_specs=in_specs, out_specs=out_specs, check_vma=False)
```

```python
import functools

import jax
import jax.numpy as jnp
from jax import lax
from jax.experimental import pallas as pl
from jax.experimental.pallas import tpu as pltpu
from jax.sharding import Mesh
from jax.sharding import PartitionSpec as P

MESH = pl.DeviceIdType.MESH
F32, BF16 = jnp.float32, jnp.bfloat16
SP = ("z", "y")
EPSILON = 1e-05
T = 256
GRID_W = 32


def silu(v):
    return (0.5 * v) * (1.0 + jnp.tanh(0.5 * v))


def dot(a, b, dims=((1,), (0,)), **kw):
    return lax.dot_general(a, b, (dims, ((), ())), preferred_element_type=F32, **kw)


def kernel(
    tok, w_inner, w_gate, w_write, w_read, w_pool, wst_in, ci_in, cc_in, rate_in, dec_in, ng_in, pmix_in,
    pg_in, woi_in, wop_in,
    out,
    x_b, hrow, hall, wa, wb1, wb2, alt1, alt3, alt4, woi, wop, de, pmix, wst, ci, cc, ng, pg, par,
    p_s, hp, y_s, v_s, b_s, c_s, cum_s, stp_s, cols_s, gate, pool, m_s,
    sb, dec, decp, st, r1, d1, pd, r2, d2, totd, res, tot, inc, b_in, own, dsend, drecv, raws, rawr, xsend, xrecv,
    mix_s, pld_s,
    lsem, ssem, rsem, psem,
):
    z, y, f, t = (lax.axis_index(a) for a in ("z", "y", "fs", "tp"))
    fq, yq, yp = lax.rem(f, 2), lax.rem(y, 2), y // 2
    r = fq * 2 + yq
    sp = z * 8 + y
    group_at = t * 2 + fq

    def along(d):
        v = lax.rem(sp + d, 64)
        return {"z": v // 8, "y": lax.rem(v, 8)}

    count = [0, 0, 0]
    sent = []

    def new(kind):
        count[kind] += 1
        return count[kind] - 1

    def start(src, dst, dev, si, ri):
        c = pltpu.make_async_remote_copy(
            src_ref=src, dst_ref=dst, send_sem=ssem.at[si], recv_sem=rsem.at[ri],
            device_id=dev, device_id_type=MESH,
        )
        c.start()
        return c

    def all_of(ref, si, ri):
        return pltpu.make_async_remote_copy(
            src_ref=ref, dst_ref=ref, send_sem=ssem.at[si], recv_sem=rsem.at[ri],
            device_id={"tp": 1 - t}, device_id_type=MESH,
        )

    def send(src, dst, dev):
        c = start(src, dst, dev, new(0), new(2))
        sent.append(c)
        return c

    def together(items, whole):
        si, ri = new(0), new(2)
        for src, dst, dev in items:
            start(src, dst, dev, si, ri)
        c = all_of(whole, si, ri)
        sent.append(c)
        return c

    def one_send(whole):
        si = new(0)
        sent.append(all_of(whole, si, 0))
        return lambda src, dst, dev: start(src, dst, dev, si, new(2))

    def local(src, dst):
        c = pltpu.make_async_copy(src, dst, lsem.at[count[1]])
        count[1] += 1
        c.start()
        return c

    def ymod(d):
        return lax.rem(y + d, 8)

    def zmod(d):
        return lax.rem(z + d, 8)

    def fmod(d):
        return lax.rem(f + d, 4)

    def pmod(d):
        return lax.rem(yp + d, 4)

    f_flip, y_flip = f + 1 - 2 * fq, y + 1 - 2 * yq
    r_x, r_y, r_d = (1 - fq) * 2 + yq, fq * 2 + 1 - yq, 3 - r
    to_x, to_y, to_d = {"fs": f_flip}, {"y": y_flip}, {"fs": f_flip, "y": y_flip}

    def at(v, n):
        return pl.ds(pl.multiple_of(v * n, n), n)

    near_first = (1, 7, 2, 6, 3, 5, 4)
    pair = {"tp": 1 - t}
    group = [pair] + [{**a, "tp": e} for a in (to_x, to_y, to_d) for e in (t, 1 - t)]
    peers = [{"y": ymod(d)} for d in range(1, 8)] + [{"z": zmod(d)} for d in range(1, 8)]
    peers += group + [{"fs": fmod(d)} for d in range(1, 4)] + [along(d) for d in (1, 63, 2, 62)]

    pool[:, 0] = jnp.zeros((2, T, 128), BF16)
    pool[:, 3] = jnp.zeros((2, T, 128), BF16)
    barrier = pltpu.get_barrier_semaphore()
    for p in peers:
        pl.semaphore_signal(barrier, inc=1, device_id=p, device_id_type=MESH)
    mine1, mine3, mine4 = (w.at[z, y] for w in (wa, wb1, wb2))
    tok_local = local(tok.at[0], x_b.at[r, t])
    w_local = [
        local(w_inner.at[:, at(q, 256)], m.at[:, pl.ds(0, 256)])
        for q, m in ((r, mine1), (r_y, alt1))
    ]
    w_local += [
        local(w.at[:, at(fq, 128)], m.at[:, pl.ds(c, 128)])
        for w, c in ((w_write, 256), (w_read, 384))
        for m in (mine1, alt1)
    ]
    w_local += [
        local(w_gate.at[:, at(r, 256)], mine3),
        local(w_gate.at[:, at(r_y, 256)], alt3),
        local(w_pool.at[:, at(r, 128)], mine4),
        local(w_pool.at[:, at(r_y, 128)], alt4),
    ]
    others = [
        local(wst_in.at[:, at(t, 16)], wst),
        local(dec_in.at[:, at(fq, 8)], de.at[r]),
        local(ci_in.at[:, at(t * 4 + r, 256)], ci),
        local(cc_in.at[:, :, at(group_at, 128)], cc),
        local(ng_in, ng),
        local(pg_in, pg),
        local(pmix_in.at[group_at, at(yq, 128)], pmix),
        local(woi_in.at[at(r, 256)], woi.at[f]),
        local(wop_in.at[at(fq, 256)], wop.at[f]),
    ]
    tok_local.wait()
    for c in w_local:
        c.wait()
    pl.semaphore_wait(barrier, len(peers))

    x_own = x_b.at[r, t]
    edges = together(
        [
            (x_own.at[pl.ds(240, 16)], hrow.at[0], along(1)),
            (x_own.at[pl.ds(0, 16)], hrow.at[1], along(63)),
        ],
        hrow,
    )

    def stage(w, mine, alt):
        items = [(alt if d % 2 else mine, mine, {"y": ymod(d)}) for d in near_first]
        return together(items, w.at[0, pl.ds(0, 7)])

    first = stage(wa, mine1, alt1)
    send_x = one_send(x_b.at[pl.ds(0, 2), 0])
    x_right = send_x(x_own, x_own, to_x)
    x_left = send_x(x_own, x_own, to_y)
    pair_i = (new(0), new(2))

    def to_pair(block):
        start(block, block, pair, *pair_i)

    x_pair = all_of(x_b.at[pl.ds(0, 3), 0], *pair_i)
    sent.append(x_pair)
    to_pair(x_own)
    decs = together(
        [
            (dec_in.at[:, at(q, 8)], de.at[r], g)
            for q, g in ((1 - fq, to_x), (fq, to_y), (1 - fq, to_d))
        ],
        de.at[pl.ds(0, 3)],
    )

    rings = {}

    def hop(piece, k, to):
        (w, a, n, only), issue = piece
        if k == 3 and only is None:
            a, n = (a if to == 1 else a + n // 2), n // 2
        s = w.at[zmod(8 - k if to == 1 else k), pl.ds(a, n)]
        return issue(s, s, {"z": zmod(to)})

    def begin(name, w, halves):
        pieces = [(w, i, 2, 1 if i < 4 else 7) for i in range(0, 8, 2)] if halves else [(w, 0, 8, None)]
        issue = one_send(w.at[pl.ds(0, 7)])
        rings[name] = [((p, issue), to, [hop((p, issue), 0, to)]) for p in pieces for to in (1, 7)]

    def step(names, k):
        for name in names:
            for piece, to, ring in rings[name]:
                last = piece[0][3] is not None and piece[0][3] != to
                if k < 4 or not last:
                    ring[k - 1].wait_recv()
                if k < 3 or (k == 3 and not last):
                    ring.append(hop(piece, k, to))

    first.wait_recv()
    begin("a", wa, True)
    edges.wait_recv()
    halo_local = local(hrow, hall.at[r * 2 + t])
    halos = together([(hrow, hall.at[r * 2 + t], g) for g in group], hall.at[pl.ds(0, 7)])
    step(("a",), 1)
    x_right.wait_recv()
    block = x_b.at[r_x, t]
    far_i = (new(0), new(2))
    x_far = all_of(x_b.at[r_d, t], *far_i)
    sent.append(x_far)
    start(block.at[pl.ds(0, 64)], block.at[pl.ds(0, 64)], to_y, *far_i)
    to_pair(block)
    x_left.wait_recv()
    block = x_b.at[r_y, t]
    start(block.at[pl.ds(64, 192)], block.at[pl.ds(64, 192)], to_x, *far_i)
    to_pair(block)
    fourth, third = stage(wb2, mine4, alt4), stage(wb1, mine3, alt3)
    step(("a",), 2)
    for c in others:
        c.wait()
    par[0:5, 0:256] = ci[...].astype(F32)
    par[0:5, 256:384] = cc[:, 0, :].astype(F32)
    par[0:5, 384:512] = cc[:, 1, :].astype(F32)
    ii = lax.broadcasted_iota(jnp.int32, (T, T), 0)
    jj = lax.broadcasted_iota(jnp.int32, (T, T), 1)
    low = lax.broadcasted_iota(jnp.int32, (T, 128), 1) < 64

    def slot_block(o):
        return lax.rem(yq + lax.rem(3 - o, 2), 2)

    def slot_unit(o):
        return lax.rem(fq + (3 - o) // 2, 2) * 2 + slot_block(o)

    r8 = lax.broadcasted_iota(jnp.int32, (8, 1), 0)
    rate = jnp.zeros((8, 1), F32)
    for i in range(8):
        rate = jnp.where(r8 == i, rate_in[i // 4, t * 16 + r * 4 + i % 4], rate)
    rate = jnp.exp(rate)

    def pick(rows, which, n):
        chosen = rows[0:4]
        for i in range(1, n):
            chosen = jnp.where(which == i, rows[4 * i : 4 * i + 4], chosen)
        return chosen

    def decay_rows(o):
        s = slot_unit(o)
        w0, w1 = wst[:, :, 0:512].reshape(32, 512), wst[:, :, 512:1024].reshape(32, 512)
        all_raw = dot(w0, x_b[s, 0], ((1,), (1,))) + dot(w1, x_b[s, 1], ((1,), (1,)))
        raw = jnp.concatenate([pick(all_raw[0:16], r, 4), pick(all_raw[16:32], r, 4)], axis=0)
        extra = jnp.concatenate([pick(de[s, 0], yq, 2), pick(de[s, 1], yq, 2)], axis=0)
        stp = jnp.maximum(raw, 0.0) + jnp.log1p(jnp.exp(-jnp.abs(raw)))
        stp_s[o] = stp
        cum_s[o] = extra - stp * rate

    x_pair.wait_recv()
    decs.wait_recv()
    for o in (3, 2, 1):
        decay_rows(o)
    step(("a",), 3)
    x_far.wait_recv()
    block = x_b.at[r_d, t]
    far_pair = send(block, block, pair)
    fourth.wait_recv()
    begin("b2", wb2, False)
    third.wait_recv()
    begin("b1", wb1, False)
    dests = [(fmod(d), lax.rem(fmod(d), 2)) for d in (1, 3, 2)]
    wos = [
        together(
            [(woi_in.at[at(q * 2 + yq, 256)], woi.at[f], {"fs": g}) for g, q in dests],
            woi.at[pl.ds(0, 3)],
        ),
        together(
            [(wop_in.at[at(q, 256)], wop.at[f], {"fs": g}) for g, q in dests], wop.at[pl.ds(0, 3)]
        ),
    ]
    far_pair.wait_recv()
    decay_rows(0)
    ld = cum_s[...].reshape(32, T)
    ld_a = ld.astype(BF16)
    rest = ld - ld_a.astype(F32)
    ld_b = rest.astype(BF16)
    ld_c = (rest - ld_b.astype(F32)).astype(BF16)
    ld3 = jnp.concatenate([ld_a, ld_b, ld_c], axis=0)
    pre = dot(ld3, (ii <= jj).astype(F32).astype(BF16))
    suf = dot(ld3, (ii >= jj).astype(F32).astype(BF16))
    pre = pre[0:32] + (pre[32:64] + pre[64:96])
    suf = suf[0:32] + (suf[32:64] + suf[64:96])
    fwd_row = lax.rem(lax.broadcasted_iota(jnp.int32, (32, T), 0), 8) < 4
    cum = jnp.where(fwd_row, pre, suf)
    cum_s[...] = cum.reshape(4, 8, T)
    lane4 = lax.broadcasted_iota(jnp.int32, (1, 256), 1) // 64
    ends = []
    for o in range(4):
        for n in range(2):
            row = jnp.zeros((1, 256), F32)
            for h in range(4):
                i = o * 8 + n * 4 + h
                e = cum[i : i + 1, T - 1 : T] if n == 0 else cum[i : i + 1, 0:1]
                row = jnp.where(lane4 == h, e, row)
            ends.append(row)
    dec[...] = jnp.concatenate(ends, axis=0)
    both = [ends[4 * hf + n] + ends[4 * hf + 2 + n] for hf in range(2) for n in range(2)]
    decp[...] = jnp.concatenate(both + [jnp.zeros((4, 256), F32)], axis=0)
    own_dec = local(decp, d1.at[yp])
    sd1 = together([(decp, d1.at[yp], {"y": ymod(2 * d)}) for d in (1, 3, 2)], d1.at[pl.ds(0, 3)])

    halo_local.wait()
    halos.wait_recv()
    step(("a",), 4)
    step(("b2",), 1)

    def rows_of(w, k, n):
        return w[4 * k : 4 * k + 4].reshape(512, n)

    halls = hall[...].reshape(4, 2, 2, 16, 512)
    h0 = halls[:, 0].reshape(128, 512)
    h1 = halls[:, 1].reshape(128, 512)
    hrow_at = lax.broadcasted_iota(jnp.int32, (128, 512), 0)
    side = lax.rem(hrow_at // 16, 2)
    place = sp - yq + lax.rem(hrow_at // 32, 2)
    gone = jnp.logical_or(
        jnp.logical_and(side == 0, place == 0), jnp.logical_and(side == 1, place == 63)
    )
    hproj = (dot(h0, rows_of(wa, 0, 512)) + dot(h1, rows_of(wa, 1, 512))).astype(BF16).astype(F32)
    hp[...] = jnp.where(gone, 0.0, hproj).reshape(4, 2, 16, 512)

    def spread(cols, c):
        parts = [
            jnp.where(low, cols[:, c + 2 * q : c + 2 * q + 1], cols[:, c + 2 * q + 1 : c + 2 * q + 2])
            for q in range(2)
        ]
        return jnp.concatenate(parts, axis=1)

    def front(o):
        s = slot_unit(o)
        x0, x1 = x_b[s, 0], x_b[s, 1]
        pa = dot(x0, rows_of(wa, 0, 512)) + dot(x1, rows_of(wa, 1, 512))
        p_s[16:272, :] = pa.astype(BF16).astype(F32)
        p_s[0:16, :] = hp[s, 0]
        p_s[272:288, :] = hp[s, 1]
        conv = p_s[14 : 14 + T, :] * par[0:1, :]
        for j in range(1, 5):
            conv = conv + p_s[14 + j : 14 + j + T, :] * par[j : j + 1, :]
        act = silu(conv)
        v, b, c = act[:, 0:256], act[:, 256:384], act[:, 384:512]
        cols = jnp.concatenate([cum_s[o], stp_s[o], jnp.zeros((112, T), F32)], axis=0).T
        cols_s[o] = cols
        v_s[o] = v.astype(BF16)
        b_s[o] = b.astype(BF16)
        c_s[o] = c.astype(BF16)
        bt = b.T.astype(BF16)
        lane = lax.broadcasted_iota(jnp.int32, (1, 128), 1)
        end = jnp.where(lane < 4, cols[T - 1 : T, :], cols[0:1, :])
        w_end = jnp.exp(end - cols)
        for n in range(2):
            scale = spread(w_end, 4 * n) * spread(cols, 8 + 4 * n)
            sb[o, n] = dot(bt, (v * scale).astype(BF16))

    def early_late(hf):
        return 2 * hf + 1 - yq, 2 * hf + yq

    def fade(o, n):
        return jnp.exp(dec[pl.ds(2 * o + n, 1), :])

    def join(hf):
        e, l = early_late(hf)
        ahead = sb[e, 0] * fade(l, 0) + sb[l, 0]
        behind = sb[l, 1] * fade(e, 1) + sb[e, 1]
        st[hf, :, 0] = ahead.astype(BF16).reshape(4, 32, 256)
        st[hf, :, 1] = behind.astype(BF16).reshape(4, 32, 256)

    def enter(hf):
        e, l = early_late(hf)
        ahead = inc[hf, :, 0].reshape(128, 256)
        behind = inc[hf, :, 1].reshape(128, 256)
        b_in[e, 0] = ahead
        b_in[l, 0] = (ahead.astype(F32) * fade(e, 0) + sb[e, 0]).astype(BF16)
        b_in[l, 1] = behind
        b_in[e, 1] = (behind.astype(F32) * fade(l, 1) + sb[l, 1]).astype(BF16)

    s1, own_st = [], []
    for hf in range(2):

        def front_step(o, _):
            front(o)
            return _

        lax.fori_loop(2 * hf, 2 * hf + 2, front_step, 0)
        join(hf)
        own_st.append(local(st.at[hf, yp], r1.at[hf, yp]))
        items = [(st.at[hf, pmod(d)], r1.at[hf, yp], {"y": ymod(2 * d)}) for d in (1, 3, 2)]
        s1.append(together(items, r1.at[hf, pl.ds(0, 3)]))
        step(("b2",), hf + 2)
        step(("b1",), hf + 1)
        if hf == 0:
            own_dec.wait()
            sd1.wait_recv()
            cumf = jnp.zeros((8, 256), F32)
            cumb = jnp.zeros((8, 256), F32)
            back = lax.rem(lax.broadcasted_iota(jnp.int32, (8, 256), 0), 2) == 1
            pf = []
            for i in range(4):
                pf.append(cumf)
                cumf = cumf + d1[i]
            for i in reversed(range(4)):
                pd[i] = jnp.exp(jnp.where(back, cumb, pf[i]))
                cumb = cumb + d1[i]
            totd[...] = cumf
            items = [(totd, d2.at[z], {"z": zmod(d)}) for d in near_first]
            sd2 = together(items, d2.at[pl.ds(0, 7)])

    def inner(o, _):
        cols, cu, stp = cols_s[o], cum_s[o], stp_s[o]
        scores = dot(c_s[o], b_s[o], ((1,), (1,)))
        for q in range(2):
            vp = v_s[o, :, q * 128 : (q + 1) * 128]
            both = []
            for e in range(2):
                h = 2 * q + e
                expo = jnp.where(
                    jj <= ii,
                    cols[:, h : h + 1] - cu[h : h + 1, :],
                    cols[:, 4 + h : 5 + h] - cu[4 + h : 5 + h, :],
                )
                df, db = stp[h : h + 1, :], stp[4 + h : 5 + h, :]
                dts = jnp.where(jj < ii, df, jnp.where(jj > ii, db, df + db))
                both.append(dot((scores * jnp.exp(expo) * dts).astype(BF16), vp))
            y_s[o, :, q * 128 : (q + 1) * 128] = jnp.where(low, both[0], both[1])
        return _

    def scan1(hf):
        own_st[hf].wait()
        s1[hf].wait_recv()
        for n in range(2):
            run = jnp.zeros((32, 256), F32)
            for i in range(4) if n == 0 else reversed(range(4)):
                res[hf, i, n] = run
                w = jnp.exp(d1[i, 2 * hf + n : 2 * hf + n + 1, :])
                run = run * w + r1[hf, i, n].astype(F32)
            tot[hf, n] = run.astype(BF16)
        items = [
            (tot.at[hf, (z + d) // 8], r2.at[hf, z, (z + d) // 8], {"z": zmod(d)})
            for d in near_first
        ]
        return together(items, r2.at[hf, pl.ds(0, 7), 0])

    def scan2(hf, s2):
        s2.wait_recv()
        for n in range(2):
            acc = jnp.zeros((32, 256), F32)
            for i in range(8) if n == 0 else reversed(range(8)):
                w = jnp.exp(d2[i, 2 * hf + n : 2 * hf + n + 1, :])
                new = acc * w + r2[hf, i, n].astype(F32)
                used = (i < z) if n == 0 else (i > z)
                acc = jnp.where(used, new, acc)
            for i in range(4):
                w = pd[i, 2 * hf + n : 2 * hf + n + 1, :]
                r1[hf, i, n] = (res[hf, i, n] + acc * w).astype(BF16)
        mine = local(r1.at[hf, yp], inc.at[hf, yp])
        items = [(r1.at[hf, pmod(d)], inc.at[hf, yp], {"y": ymod(2 * d)}) for d in (1, 3, 2)]
        return mine, together(items, inc.at[hf, pl.ds(0, 3)])

    def gates(o, _):
        s = slot_unit(o)
        g = dot(x_b[s, 0], rows_of(wb1, 0, 256)) + dot(x_b[s, 1], rows_of(wb1, 1, 256))
        gate[o] = silu(g.astype(BF16).astype(F32))
        return _

    def grids(o, _):
        s = slot_unit(o)
        q = dot(x_b[s, 0], rows_of(wb2, 0, 128)) + dot(x_b[s, 1], rows_of(wb2, 1, 128))
        pool[o // 2, 1 + slot_block(o)] = q.astype(BF16)
        return _

    def pool_copies(g):
        n = GRID_W << g
        spans = ((2, 0, T - n, along(2)), (1, 3, 0, along(62)))
        return [
            pltpu.make_async_remote_copy(
                src_ref=pool.at[:, a, pl.ds(c, n)], dst_ref=pool.at[:, b, pl.ds(c, n)],
                send_sem=psem.at[0, i], recv_sem=psem.at[1, i], device_id=dev, device_id_type=MESH,
            )
            for i, (a, b, c, dev) in enumerate(spans)
        ]

    lax.fori_loop(0, 2, inner, 0)
    k = jnp.left_shift(jnp.int32(2), group_at)
    ti = lax.broadcasted_iota(jnp.int32, (T, 3 * T), 0)
    tj = lax.broadcasted_iota(jnp.int32, (T, 3 * T), 1)
    ri, ci_ = ti // GRID_W + 8, lax.rem(ti, GRID_W)
    rj, cj = tj // GRID_W, lax.rem(tj, GRID_W)
    inside = (rj >= ri - k // 2) & (rj < ri + k // 2) & (cj >= ci_ - k // 2) & (cj < ci_ + k // 2)
    m_s[...] = inside.astype(F32).astype(BF16)
    s2_0 = scan1(0)
    step(("b2",), 4)
    lax.fori_loop(0, 4, grids, 0)
    for g in range(4):

        @pl.when(group_at == g)
        def _():
            for c in pool_copies(g):
                c.start()

    step(("b1",), 3)
    lax.fori_loop(2, 4, inner, 0)
    s2_1 = scan1(1)
    sd2.wait_recv()
    s3_0 = scan2(0, s2_0)
    step(("b1",), 4)
    lax.fori_loop(0, 4, gates, 0)
    s3_1 = scan2(1, s2_1)

    for g in range(4):

        @pl.when(group_at == g)
        def _():
            for c in pool_copies(g):
                c.wait()
    pool[:, 0] = jnp.where(sp // 2 == 0, jnp.zeros((2, T, 128), BF16), pool[:, 0])
    pool[:, 3] = jnp.where(sp // 2 == 31, jnp.zeros((2, T, 128), BF16), pool[:, 3])
    col = lax.rem(lax.broadcasted_iota(jnp.int32, (T, 128), 0), GRID_W)
    cols_in = jnp.minimum(col + k // 2, GRID_W) - jnp.maximum(col - k // 2, 0)
    pgain = jnp.concatenate([pg[pl.ds(2 * group_at + i, 1), :] for i in range(2)], axis=1)
    ngain = jnp.concatenate([ng[pl.ds(8 * t + 2 * r + i, 1), :] for i in range(2)], axis=1)

    def pools(o, _):
        b = slot_block(o)
        row = lax.broadcasted_iota(jnp.int32, (T, 128), 0) // GRID_W + (sp - yq + b) * 8
        cells = (jnp.minimum(row + k // 2, 512) - jnp.maximum(row - k // 2, 0)) * cols_in
        rows = jnp.concatenate([pool[o // 2, b + i] for i in range(3)], axis=0)
        off = dot(m_s[...], rows) / cells.astype(F32) - pool[o // 2, b + 1].astype(F32)
        pld_s[o] = (dot(off.astype(BF16), pmix[...]) * pgain).astype(BF16)
        return _

    lax.fori_loop(0, 4, pools, 0)

    for c in wos:
        c.wait_recv()
    blk = ((ii // 64 == jj // 64).astype(F32) * (1.0 / 64.0)).astype(BF16)

    def finish(o):
        cb, cols = c_s[o], jnp.exp(cols_s[o])
        carried = dot(cb, b_in[o, 0]) * spread(cols, 0) + dot(cb, b_in[o, 1]) * spread(cols, 4)
        g = (y_s[o] + carried) * gate[o]
        ms = dot((g * g).astype(BF16), blk)
        mix_s[...] = (g * lax.rsqrt(ms + EPSILON) * ngain).astype(BF16)

    mine = at(t, 128)
    theirs = at(1 - t, 128)
    swaps = []
    swap_send = one_send(dsend)
    raw_send = one_send(raws)
    out_i = (new(0), new(2))
    far = all_of(xrecv, *out_i)
    sent.append(far)

    def produce(o):
        finish(o)
        for q in range(4):
            cs = slice(q * 256, (q + 1) * 256)
            part = dot(mix_s[theirs, :], woi[q]) + dot(pld_s[o, theirs, :], wop[q])
            dsend[o, :, cs] = part.astype(BF16)
        swaps.append(swap_send(dsend.at[o], drecv.at[o], pair))
        for q in range(4):
            cs = slice(q * 256, (q + 1) * 256)
            own[o, :, cs] = dot(mix_s[mine, :], woi[q]) + dot(pld_s[o, mine, :], wop[q])

    def chip_sum(o):
        swaps[o].wait_recv()
        return (own[o] + drecv[o].astype(F32)).reshape(2, 64, 1024)

    def arrive(hf, s3):
        s3[0].wait()
        s3[1].wait_recv()
        enter(hf)

    def out_half(i, h, value, dev, a=0):
        n = value.shape[0]
        xsend[i, h, a : a + n] = value.astype(BF16)
        rows = pl.ds(a, n)
        start(xsend.at[i, h, rows], xrecv.at[i, h, rows], dev, *out_i)

    arrive(0, s3_0)
    produce(0)
    produce(1)
    raws[...] = chip_sum(0).astype(BF16)
    up, down = [], []
    for q in range(2):
        rows = pl.ds(q * 32, 32)
        up.append(raw_send(raws.at[0, rows], rawr.at[0, rows], to_x))
        down.append(raw_send(raws.at[1, rows], rawr.at[1, rows], to_y))
    chip1 = chip_sum(1)
    out_half(0, 0, chip1[0], to_x)
    own[1, 64:128] = chip1[1]
    arrive(1, s3_1)
    produce(2)
    produce(3)
    chip2 = chip_sum(2)
    out_half(1, 1, chip2[1], to_y)
    for q in range(2):
        a = q * 32
        down[q].wait_recv()
        out_half(0, 1, own[1, 64 + a : 96 + a] + rawr[1, a : a + 32].astype(F32), to_x, a)
        up[q].wait_recv()
        out_half(1, 0, chip2[0, a : a + 32] + rawr[0, a : a + 32].astype(F32), to_y, a)
    own[3] = chip_sum(3).reshape(128, 1024)
    far.wait_recv()
    arrived = (xrecv[0].astype(F32) + xrecv[1].astype(F32)).reshape(128, 1024)
    out[0] = (own[3] + arrived).astype(BF16)
    for c in sent:
        c.wait_send()


N_LOCAL, N_SEND, N_RECV = 26, 26, 74


def body(
    tokens, w_inner, w_gate, w_write, w_read, w_pool_in, w_step, conv_inner, conv_cross, rate_log,
    decay_extra, norm_gain, pool_mix, pool_gain, w_out_inner, w_out_pool,
):
    hbm = pl.BlockSpec(memory_space=pl.ANY)
    V = pltpu.VMEM
    scratch = [
        V((4, 2, T, 512), BF16),
        V((2, 16, 512), BF16),
        V((8, 2, 16, 512), BF16),
        V((8, 8, 16, 512), BF16),
        V((8, 8, 16, 256), BF16),
        V((8, 8, 16, 128), BF16),
        V((16, 512), BF16),
        V((16, 256), BF16),
        V((16, 128), BF16),
        V((4, 256, 256), BF16),
        V((4, 256, 256), BF16),
        V((4, 2, 8, T), F32),
        V((128, 256), BF16),
        V((2, 16, 1024), BF16),
        V((5, 256), BF16),
        V((5, 2, 128), BF16),
        V((16, 128), F32),
        V((8, 128), F32),
        V((8, 512), F32),
        V((288, 512), F32),
        V((4, 2, 16, 512), F32),
        V((4, T, 256), F32),
        V((4, T, 256), BF16),
        V((4, T, 128), BF16),
        V((4, T, 128), BF16),
        V((4, 8, T), F32),
        V((4, 8, T), F32),
        V((4, T, 128), F32),
        V((4, T, 256), F32),
        V((2, 4, T, 128), BF16),
        V((T, 3 * T), BF16),
        V((4, 2, 128, 256), F32),
        V((8, 256), F32),
        V((8, 256), F32),
        V((2, 4, 2, 32, 256), BF16),
        V((2, 4, 2, 32, 256), BF16),
        V((4, 8, 256), F32),
        V((4, 8, 256), F32),
        V((2, 8, 2, 32, 256), BF16),
        V((8, 8, 256), F32),
        V((8, 256), F32),
        V((2, 4, 2, 32, 256), F32),
        V((2, 2, 32, 256), BF16),
        V((2, 4, 2, 32, 256), BF16),
        V((4, 2, 128, 256), BF16),
        V((4, 128, 1024), F32),
        V((4, 128, 1024), BF16),
        V((4, 128, 1024), BF16),
        V((2, 64, 1024), BF16),
        V((2, 64, 1024), BF16),
        V((2, 2, 64, 1024), BF16),
        V((2, 2, 64, 1024), BF16),
        V((T, 256), BF16),
        V((4, T, 256), BF16),
        pltpu.SemaphoreType.DMA((N_LOCAL,)),
        pltpu.SemaphoreType.DMA((N_SEND,)),
        pltpu.SemaphoreType.DMA((N_RECV,)),
        pltpu.SemaphoreType.DMA((2, 2)),
    ]
    return pl.pallas_call(
        kernel,
        out_shape=jax.ShapeDtypeStruct((1, 128, 1024), BF16),
        in_specs=[hbm] * 9 + [pl.BlockSpec(memory_space=pltpu.SMEM)] + [hbm] * 6,
        out_specs=pl.BlockSpec(memory_space=pltpu.VMEM),
        scratch_shapes=scratch,
        compiler_params=pltpu.CompilerParams(
            collective_id=0, has_side_effects=True, vmem_limit_bytes=60 * 1024 * 1024
        ),
    )(
        tokens, w_inner, w_gate, w_write, w_read, w_pool_in, jnp.transpose(w_step, (1, 2, 0)),
        conv_inner, conv_cross, rate_log, jnp.transpose(decay_extra[0], (1, 2, 0)),
        norm_gain.reshape(16, 128), pool_mix, pool_gain.reshape(8, 128), w_out_inner, w_out_pool,
    )


def solution(mesh):
    finer = Mesh(
        mesh.devices.reshape(8, 8, mesh.shape["fs"], mesh.shape["tp"]), ("z", "y", "fs", "tp")
    )
    in_specs = (
        P("fs", SP, "tp"),
        P(SP, "tp"),
        P(SP, "tp"),
        P(SP, "tp"),
        P(SP, "tp"),
        P(SP, "tp"),
        P(),
        P(),
        P(),
        P(),
        P("fs", SP, None, "tp"),
        P(),
        P(),
        P(),
        P("tp", "fs"),
        P("tp", "fs"),
    )
    out_specs = P("fs", ("z", "y", "tp"), None)
    return jax.shard_map(body, mesh=finer, in_specs=in_specs, out_specs=out_specs, check_vma=False)
```

```python
import functools

import jax
import jax.numpy as jnp
from jax import lax
from jax.experimental import pallas as pl
from jax.experimental.pallas import tpu as pltpu
from jax.sharding import Mesh
from jax.sharding import PartitionSpec as P

MESH = pl.DeviceIdType.MESH
F32, BF16 = jnp.float32, jnp.bfloat16
SP = ("z", "y")
EPSILON = 1e-05
T = 256
GRID_W = 32


def silu(v):
    return (0.5 * v) * (1.0 + jnp.tanh(0.5 * v))


def dot(a, b, dims=((1,), (0,)), **kw):
    return lax.dot_general(a, b, (dims, ((), ())), preferred_element_type=F32, **kw)


def kernel(
    tok, w_inner, w_gate, w_write, w_read, w_pool, wst_in, ci_in, cc_in, rate_in, dec_in, ng_in, pmix_in,
    pg_in, woi_in, wop_in,
    out,
    x_b, hrow, hall, wa, wb1, wb2, alt1, alt3, alt4, woi, wop, de, pmix, wst, rate_s, ci, cc, ng, pg, par,
    p_s, p_r, hp, y_s, v_s, b_s, c_s, cum_s, stp_s, cols_s, gate, pool, m_s,
    sb, dec, decp, st, r1, d1, pd, r2, d2, totd, res, tot, inc, b_in, own, dsend, drecv, raws, rawr, xsend, xrecv,
    mix_s, pld_s,
    lsem, ssem, rsem, psem,
):
    z, y, f, t = (lax.axis_index(a) for a in ("z", "y", "fs", "tp"))
    fq, yq, yp = lax.rem(f, 2), lax.rem(y, 2), y // 2
    r = fq * 2 + yq
    sp = z * 8 + y
    group_at = t * 2 + fq

    def along(d):
        v = lax.rem(sp + d, 64)
        return {"z": v // 8, "y": lax.rem(v, 8)}

    count = [0, 0, 0]
    sent = []

    def new(kind):
        count[kind] += 1
        return count[kind] - 1

    def start(src, dst, dev, si, ri):
        c = pltpu.make_async_remote_copy(
            src_ref=src, dst_ref=dst, send_sem=ssem.at[si], recv_sem=rsem.at[ri],
            device_id=dev, device_id_type=MESH,
        )
        c.start()
        return c

    def all_of(ref, si, ri):
        return pltpu.make_async_remote_copy(
            src_ref=ref, dst_ref=ref, send_sem=ssem.at[si], recv_sem=rsem.at[ri],
            device_id={"tp": 1 - t}, device_id_type=MESH,
        )

    def send(src, dst, dev):
        c = start(src, dst, dev, new(0), new(2))
        sent.append(c)
        return c

    def together(items, whole):
        si, ri = new(0), new(2)
        for src, dst, dev in items:
            start(src, dst, dev, si, ri)
        c = all_of(whole, si, ri)
        sent.append(c)
        return c

    def one_send(whole):
        si = new(0)
        sent.append(all_of(whole, si, 0))
        return lambda src, dst, dev: start(src, dst, dev, si, new(2))

    def local(src, dst):
        c = pltpu.make_async_copy(src, dst, lsem.at[count[1]])
        count[1] += 1
        c.start()
        return c

    def ymod(d):
        return lax.rem(y + d, 8)

    def zmod(d):
        return lax.rem(z + d, 8)

    def fmod(d):
        return lax.rem(f + d, 4)

    def pmod(d):
        return lax.rem(yp + d, 4)

    f_flip, y_flip = f + 1 - 2 * fq, y + 1 - 2 * yq
    r_x, r_y, r_d = (1 - fq) * 2 + yq, fq * 2 + 1 - yq, 3 - r
    to_x, to_y, to_d = {"fs": f_flip}, {"y": y_flip}, {"fs": f_flip, "y": y_flip}

    def at(v, n):
        return pl.ds(pl.multiple_of(v * n, n), n)

    near_first = (1, 7, 2, 6, 3, 5, 4)
    pair = {"tp": 1 - t}
    group = [pair] + [{**a, "tp": e} for a in (to_x, to_y, to_d) for e in (t, 1 - t)]
    peers = [{"y": ymod(d)} for d in range(1, 8)] + [{"z": zmod(d)} for d in range(1, 8)]
    peers += group + [{"fs": fmod(d)} for d in range(1, 4)] + [along(d) for d in (1, 63, 2, 62)]

    barrier = pltpu.get_barrier_semaphore()
    for p in peers:
        pl.semaphore_signal(barrier, inc=1, device_id=p, device_id_type=MESH)
    mine1, mine3, mine4 = (w.at[z, y] for w in (wa, wb1, wb2))
    tok_local = local(tok.at[0], x_b.at[r, t])
    w_local = [
        local(w_inner.at[:, at(q, 256)], m.at[:, pl.ds(0, 256)])
        for q, m in ((r, mine1), (r_y, alt1))
    ]
    w_local += [
        local(w.at[:, at(fq, 128)], m.at[:, pl.ds(c, 128)])
        for w, c in ((w_write, 256), (w_read, 384))
        for m in (mine1, alt1)
    ]
    w_local += [
        local(w_gate.at[:, at(r, 256)], mine3),
        local(w_gate.at[:, at(r_y, 256)], alt3),
        local(w_pool.at[:, at(r, 128)], mine4),
        local(w_pool.at[:, at(r_y, 128)], alt4),
    ]
    others = [
        local(wst_in.at[:, at(t, 16)], wst),
        local(dec_in.at[:, at(fq, 8)], de.at[r]),
        local(ci_in.at[:, at(t * 4 + r, 256)], ci),
        local(cc_in.at[:, :, at(group_at, 128)], cc),
        local(ng_in, ng),
        local(rate_in, rate_s),
        local(pg_in, pg),
        local(pmix_in.at[group_at, at(yq, 128)], pmix),
        local(woi_in.at[at(r, 256)], woi.at[f]),
        local(wop_in.at[at(fq, 256)], wop.at[f]),
    ]
    pool[:, 0] = jnp.zeros((2, T, 128), BF16)
    pool[:, 3] = jnp.zeros((2, T, 128), BF16)
    tok_local.wait()
    for c in w_local:
        c.wait()
    pl.semaphore_wait(barrier, len(peers))

    x_own = x_b.at[r, t]
    edges = together(
        [
            (x_own.at[pl.ds(240, 16)], hrow.at[0], along(1)),
            (x_own.at[pl.ds(0, 16)], hrow.at[1], along(63)),
        ],
        hrow,
    )

    def stage(w, mine, alt):
        items = [(alt if d % 2 else mine, mine, {"y": ymod(d)}) for d in near_first]
        return together(items, w.at[0, pl.ds(0, 7)])

    first = stage(wa, mine1, alt1)
    send_x = one_send(x_b.at[pl.ds(0, 2), 0])
    x_right = send_x(x_own, x_own, to_x)
    x_left = send_x(x_own, x_own, to_y)
    pair_i = (new(0), new(2))

    def to_pair(block):
        start(block, block, pair, *pair_i)

    x_pair = all_of(x_b.at[pl.ds(0, 3), 0], *pair_i)
    sent.append(x_pair)
    to_pair(x_own)
    decs = together(
        [
            (dec_in.at[:, at(q, 8)], de.at[r], g)
            for q, g in ((1 - fq, to_x), (fq, to_y), (1 - fq, to_d))
        ],
        de.at[pl.ds(0, 3)],
    )

    rings = {}

    def hop(piece, k, to):
        (w, a, n, only), issue = piece
        if k == 3 and only is None:
            a, n = (a if to == 1 else a + n // 2), n // 2
        s = w.at[zmod(8 - k if to == 1 else k), pl.ds(a, n)]
        return issue(s, s, {"z": zmod(to)})

    def begin(name, w, halves):
        pieces = [(w, i, 2, 1 if i < 4 else 7) for i in range(0, 8, 2)] if halves else [(w, 0, 8, None)]
        issue = one_send(w.at[pl.ds(0, 7)])
        rings[name] = [((p, issue), to, [hop((p, issue), 0, to)]) for p in pieces for to in (1, 7)]

    def step(names, k):
        for name in names:
            for piece, to, ring in rings[name]:
                last = piece[0][3] is not None and piece[0][3] != to
                if k < 4 or not last:
                    ring[k - 1].wait_recv()
                if k < 3 or (k == 3 and not last):
                    ring.append(hop(piece, k, to))

    first.wait_recv()
    begin("a", wa, True)
    edges.wait_recv()
    halo_local = local(hrow, hall.at[r * 2 + t])
    halos = together([(hrow, hall.at[r * 2 + t], g) for g in group], hall.at[pl.ds(0, 7)])
    step(("a",), 1)
    x_right.wait_recv()
    block = x_b.at[r_x, t]
    far_i = (new(0), new(2))
    x_far = all_of(x_b.at[r_d, t], *far_i)
    sent.append(x_far)
    start(block.at[pl.ds(0, 64)], block.at[pl.ds(0, 64)], to_y, *far_i)
    to_pair(block)
    x_left.wait_recv()
    block = x_b.at[r_y, t]
    start(block.at[pl.ds(64, 192)], block.at[pl.ds(64, 192)], to_x, *far_i)
    to_pair(block)
    fourth, third = stage(wb2, mine4, alt4), stage(wb1, mine3, alt3)
    step(("a",), 2)
    for c in others:
        c.wait()
    par[0:5, 0:256] = ci[...].astype(F32)
    par[0:5, 256:384] = cc[:, 0, :].astype(F32)
    par[0:5, 384:512] = cc[:, 1, :].astype(F32)
    ii = lax.broadcasted_iota(jnp.int32, (T, T), 0)
    jj = lax.broadcasted_iota(jnp.int32, (T, T), 1)
    low = lax.broadcasted_iota(jnp.int32, (T, 128), 1) < 64

    def slot_block(o):
        return lax.rem(yq + lax.rem(3 - o, 2), 2)

    def slot_unit(o):
        return lax.rem(fq + (3 - o) // 2, 2) * 2 + slot_block(o)

    r8 = lax.broadcasted_iota(jnp.int32, (8, 1), 0)
    rate = jnp.zeros((8, 1), F32)
    for i in range(8):
        rate = jnp.where(r8 == i, rate_s[i // 4, t * 16 + r * 4 + i % 4], rate)
    rate = jnp.exp(rate)

    def pick(rows, which, n):
        chosen = rows[0:4]
        for i in range(1, n):
            chosen = jnp.where(which == i, rows[4 * i : 4 * i + 4], chosen)
        return chosen

    def decay_rows(o):
        s = slot_unit(o)
        w0, w1 = wst[:, :, 0:512].reshape(32, 512), wst[:, :, 512:1024].reshape(32, 512)
        all_raw = dot(w0, x_b[s, 0], ((1,), (1,))) + dot(w1, x_b[s, 1], ((1,), (1,)))
        raw = jnp.concatenate([pick(all_raw[0:16], r, 4), pick(all_raw[16:32], r, 4)], axis=0)
        extra = jnp.concatenate([pick(de[s, 0], yq, 2), pick(de[s, 1], yq, 2)], axis=0)
        stp = jnp.maximum(raw, 0.0) + jnp.log1p(jnp.exp(-jnp.abs(raw)))
        stp_s[o] = stp
        cum_s[o] = extra - stp * rate

    x_pair.wait_recv()
    decs.wait_recv()
    for o in (3, 2, 1):
        decay_rows(o)
    step(("a",), 3)
    x_far.wait_recv()
    block = x_b.at[r_d, t]
    far_pair = send(block, block, pair)
    fourth.wait_recv()
    begin("b2", wb2, False)
    third.wait_recv()
    begin("b1", wb1, False)
    dests = [(fmod(d), lax.rem(fmod(d), 2)) for d in (1, 3, 2)]
    wos = [
        together(
            [(woi_in.at[at(q * 2 + yq, 256)], woi.at[f], {"fs": g}) for g, q in dests],
            woi.at[pl.ds(0, 3)],
        ),
        together(
            [(wop_in.at[at(q, 256)], wop.at[f], {"fs": g}) for g, q in dests], wop.at[pl.ds(0, 3)]
        ),
    ]
    far_pair.wait_recv()
    decay_rows(0)
    ld = cum_s[...].reshape(32, T)
    ld_a = ld.astype(BF16)
    rest = ld - ld_a.astype(F32)
    ld_b = rest.astype(BF16)
    ld_c = (rest - ld_b.astype(F32)).astype(BF16)
    ld3 = jnp.concatenate([ld_a, ld_b, ld_c], axis=0)
    pre = dot(ld3, (ii <= jj).astype(F32).astype(BF16))
    suf = dot(ld3, (ii >= jj).astype(F32).astype(BF16))
    pre = pre[0:32] + (pre[32:64] + pre[64:96])
    suf = suf[0:32] + (suf[32:64] + suf[64:96])
    fwd_row = lax.rem(lax.broadcasted_iota(jnp.int32, (32, T), 0), 8) < 4
    cum = jnp.where(fwd_row, pre, suf)
    cum_s[...] = cum.reshape(4, 8, T)
    lane4 = lax.broadcasted_iota(jnp.int32, (1, 256), 1) // 64
    ends = []
    for o in range(4):
        for n in range(2):
            row = jnp.zeros((1, 256), F32)
            for h in range(4):
                i = o * 8 + n * 4 + h
                e = cum[i : i + 1, T - 1 : T] if n == 0 else cum[i : i + 1, 0:1]
                row = jnp.where(lane4 == h, e, row)
            ends.append(row)
    dec[...] = jnp.concatenate(ends, axis=0)
    both = [ends[4 * hf + n] + ends[4 * hf + 2 + n] for hf in range(2) for n in range(2)]
    decp[...] = jnp.concatenate(both + [jnp.zeros((4, 256), F32)], axis=0)
    own_dec = local(decp, d1.at[yp])
    sd1 = together([(decp, d1.at[yp], {"y": ymod(2 * d)}) for d in (1, 3, 2)], d1.at[pl.ds(0, 3)])

    halo_local.wait()
    halos.wait_recv()
    step(("a",), 4)
    step(("b2",), 1)

    def rows_of(w, k, n):
        return w[4 * k : 4 * k + 4].reshape(512, n)

    halls = hall[...].reshape(4, 2, 2, 16, 512)
    h0 = halls[:, 0].reshape(128, 512)
    h1 = halls[:, 1].reshape(128, 512)
    hrow_at = lax.broadcasted_iota(jnp.int32, (128, 512), 0)
    side = lax.rem(hrow_at // 16, 2)
    place = sp - yq + lax.rem(hrow_at // 32, 2)
    gone = jnp.logical_or(
        jnp.logical_and(side == 0, place == 0), jnp.logical_and(side == 1, place == 63)
    )
    hproj = (dot(h0, rows_of(wa, 0, 512)) + dot(h1, rows_of(wa, 1, 512))).astype(BF16).astype(F32)
    hp[...] = jnp.where(gone, 0.0, hproj).reshape(4, 2, 16, 512)

    def spread(cols, c):
        parts = [
            jnp.where(low, cols[:, c + 2 * q : c + 2 * q + 1], cols[:, c + 2 * q + 1 : c + 2 * q + 2])
            for q in range(2)
        ]
        return jnp.concatenate(parts, axis=1)

    def convolve(s, x0, x1, buf, c, n):
        cs = slice(c, c + n)
        w0, w1 = (wa[4 * k : 4 * k + 4, :, :, cs].reshape(512, n) for k in range(2))
        buf[16:272, :] = (dot(x0, w0) + dot(x1, w1)).astype(BF16).astype(F32)
        buf[0:16, :] = hp[s, 0, :, cs]
        buf[272:288, :] = hp[s, 1, :, cs]
        conv = buf[14 : 14 + T, :] * par[0:1, cs]
        for j in range(1, 5):
            conv = conv + buf[14 + j : 14 + j + T, :] * par[j : j + 1, cs]
        return silu(conv)

    def front(o):
        s = slot_unit(o)
        x0, x1 = x_b[s, 0], x_b[s, 1]
        act = convolve(s, x0, x1, p_s, 0, 384)
        v, b = act[:, 0:256], act[:, 256:384]
        cols = jnp.concatenate([cum_s[o], stp_s[o], jnp.zeros((112, T), F32)], axis=0).T
        cols_s[o] = cols
        v_s[o] = v.astype(BF16)
        b_s[o] = b.astype(BF16)
        bt = b.T.astype(BF16)
        lane = lax.broadcasted_iota(jnp.int32, (1, 128), 1)
        end = jnp.where(lane < 4, cols[T - 1 : T, :], cols[0:1, :])
        w_end = jnp.exp(end - cols)
        for n in range(2):
            scale = spread(w_end, 4 * n) * spread(cols, 8 + 4 * n)
            sb[o, n] = dot(bt, (v * scale).astype(BF16))

    def early_late(hf):
        return 2 * hf + 1 - yq, 2 * hf + yq

    def fade(o, n):
        return jnp.exp(dec[pl.ds(2 * o + n, 1), :])

    def join(hf):
        e, l = early_late(hf)
        ahead = sb[e, 0] * fade(l, 0) + sb[l, 0]
        behind = sb[l, 1] * fade(e, 1) + sb[e, 1]
        st[hf, :, 0] = ahead.astype(BF16).reshape(4, 32, 256)
        st[hf, :, 1] = behind.astype(BF16).reshape(4, 32, 256)

    def enter(hf):
        e, l = early_late(hf)
        ahead = inc[hf, :, 0].reshape(128, 256)
        behind = inc[hf, :, 1].reshape(128, 256)
        b_in[e, 0] = ahead
        b_in[l, 0] = (ahead.astype(F32) * fade(e, 0) + sb[e, 0]).astype(BF16)
        b_in[l, 1] = behind
        b_in[e, 1] = (behind.astype(F32) * fade(l, 1) + sb[l, 1]).astype(BF16)

    s1, own_st = [], []
    for hf in range(2):

        def front_step(o, _):
            front(o)
            return _

        lax.fori_loop(2 * hf, 2 * hf + 2, front_step, 0)
        join(hf)
        own_st.append(local(st.at[hf, yp], r1.at[hf, yp]))
        items = [(st.at[hf, pmod(d)], r1.at[hf, yp], {"y": ymod(2 * d)}) for d in (1, 3, 2)]
        s1.append(together(items, r1.at[hf, pl.ds(0, 3)]))
        step(("b2",), hf + 2)
        step(("b1",), hf + 1)
        if hf == 0:
            own_dec.wait()
            sd1.wait_recv()
            cumf = jnp.zeros((8, 256), F32)
            cumb = jnp.zeros((8, 256), F32)
            back = lax.rem(lax.broadcasted_iota(jnp.int32, (8, 256), 0), 2) == 1
            pf = []
            for i in range(4):
                pf.append(cumf)
                cumf = cumf + d1[i]
            for i in reversed(range(4)):
                pd[i] = jnp.exp(jnp.where(back, cumb, pf[i]))
                cumb = cumb + d1[i]
            totd[...] = cumf
            items = [(totd, d2.at[z], {"z": zmod(d)}) for d in near_first]
            sd2 = together(items, d2.at[pl.ds(0, 7)])

    def inner(o, _):
        s = slot_unit(o)
        c_s[o] = convolve(s, x_b[s, 0], x_b[s, 1], p_r, 384, 128).astype(BF16)
        cols, cu, stp = cols_s[o], cum_s[o], stp_s[o]
        scores = dot(c_s[o], b_s[o], ((1,), (1,)))
        for q in range(2):
            vp = v_s[o, :, q * 128 : (q + 1) * 128]
            both = []
            for e in range(2):
                h = 2 * q + e
                expo = jnp.where(
                    jj <= ii,
                    cols[:, h : h + 1] - cu[h : h + 1, :],
                    cols[:, 4 + h : 5 + h] - cu[4 + h : 5 + h, :],
                )
                df, db = stp[h : h + 1, :], stp[4 + h : 5 + h, :]
                dts = jnp.where(jj < ii, df, jnp.where(jj > ii, db, df + db))
                both.append(dot((scores * jnp.exp(expo) * dts).astype(BF16), vp))
            y_s[o, :, q * 128 : (q + 1) * 128] = jnp.where(low, both[0], both[1])
        return _

    def scan1(hf):
        own_st[hf].wait()
        s1[hf].wait_recv()
        for n in range(2):
            run = jnp.zeros((32, 256), F32)
            for i in range(4) if n == 0 else reversed(range(4)):
                res[hf, i, n] = run
                w = jnp.exp(d1[i, 2 * hf + n : 2 * hf + n + 1, :])
                run = run * w + r1[hf, i, n].astype(F32)
            tot[hf, n] = run.astype(BF16)
        items = [
            (tot.at[hf, (z + d) // 8], r2.at[hf, z, (z + d) // 8], {"z": zmod(d)})
            for d in near_first
        ]
        return together(items, r2.at[hf, pl.ds(0, 7), 0])

    def scan2(hf, s2):
        s2.wait_recv()
        for n in range(2):
            acc = jnp.zeros((32, 256), F32)
            for i in range(8) if n == 0 else reversed(range(8)):
                w = jnp.exp(d2[i, 2 * hf + n : 2 * hf + n + 1, :])
                new = acc * w + r2[hf, i, n].astype(F32)
                used = (i < z) if n == 0 else (i > z)
                acc = jnp.where(used, new, acc)
            for i in range(4):
                w = pd[i, 2 * hf + n : 2 * hf + n + 1, :]
                r1[hf, i, n] = (res[hf, i, n] + acc * w).astype(BF16)
        mine = local(r1.at[hf, yp], inc.at[hf, yp])
        items = [(r1.at[hf, pmod(d)], inc.at[hf, yp], {"y": ymod(2 * d)}) for d in (1, 3, 2)]
        return mine, together(items, inc.at[hf, pl.ds(0, 3)])

    def gates(o, _):
        s = slot_unit(o)
        g = dot(x_b[s, 0], rows_of(wb1, 0, 256)) + dot(x_b[s, 1], rows_of(wb1, 1, 256))
        gate[o] = silu(g.astype(BF16).astype(F32))
        return _

    def grids(o, _):
        s = slot_unit(o)
        q = dot(x_b[s, 0], rows_of(wb2, 0, 128)) + dot(x_b[s, 1], rows_of(wb2, 1, 128))
        pool[o // 2, 1 + slot_block(o)] = q.astype(BF16)
        return _

    def pool_copies(g):
        n = GRID_W << g
        spans = ((2, 0, T - n, along(2)), (1, 3, 0, along(62)))
        return [
            pltpu.make_async_remote_copy(
                src_ref=pool.at[:, a, pl.ds(c, n)], dst_ref=pool.at[:, b, pl.ds(c, n)],
                send_sem=psem.at[0, i], recv_sem=psem.at[1, i], device_id=dev, device_id_type=MESH,
            )
            for i, (a, b, c, dev) in enumerate(spans)
        ]

    lax.fori_loop(0, 2, inner, 0)
    k = jnp.left_shift(jnp.int32(2), group_at)
    ti = lax.broadcasted_iota(jnp.int32, (T, 3 * T), 0)
    tj = lax.broadcasted_iota(jnp.int32, (T, 3 * T), 1)
    ri, ci_ = ti // GRID_W + 8, lax.rem(ti, GRID_W)
    rj, cj = tj // GRID_W, lax.rem(tj, GRID_W)
    inside = (rj >= ri - k // 2) & (rj < ri + k // 2) & (cj >= ci_ - k // 2) & (cj < ci_ + k // 2)
    m_s[...] = inside.astype(F32).astype(BF16)
    s2_0 = scan1(0)
    step(("b2",), 4)
    lax.fori_loop(0, 4, grids, 0)
    for g in range(4):

        @pl.when(group_at == g)
        def _():
            for c in pool_copies(g):
                c.start()

    step(("b1",), 3)
    lax.fori_loop(2, 4, inner, 0)
    s2_1 = scan1(1)
    sd2.wait_recv()
    s3_0 = scan2(0, s2_0)
    step(("b1",), 4)
    lax.fori_loop(0, 4, gates, 0)
    for g in range(4):

        @pl.when(group_at == g)
        def _():
            for c in pool_copies(g):
                c.wait()
    pool[:, 0] = jnp.where(sp // 2 == 0, jnp.zeros((2, T, 128), BF16), pool[:, 0])
    pool[:, 3] = jnp.where(sp // 2 == 31, jnp.zeros((2, T, 128), BF16), pool[:, 3])
    col = lax.rem(lax.broadcasted_iota(jnp.int32, (T, 128), 0), GRID_W)
    cols_in = jnp.minimum(col + k // 2, GRID_W) - jnp.maximum(col - k // 2, 0)
    pgain = jnp.concatenate([pg[pl.ds(2 * group_at + i, 1), :] for i in range(2)], axis=1)
    ngain = jnp.concatenate([ng[pl.ds(8 * t + 2 * r + i, 1), :] for i in range(2)], axis=1)

    def pools(o, _):
        b = slot_block(o)
        row = lax.broadcasted_iota(jnp.int32, (T, 128), 0) // GRID_W + (sp - yq + b) * 8
        cells = (jnp.minimum(row + k // 2, 512) - jnp.maximum(row - k // 2, 0)) * cols_in
        rows = jnp.concatenate([pool[o // 2, b + i] for i in range(3)], axis=0)
        off = dot(m_s[...], rows) / cells.astype(F32) - pool[o // 2, b + 1].astype(F32)
        pld_s[o] = (dot(off.astype(BF16), pmix[...]) * pgain).astype(BF16)
        return _

    lax.fori_loop(0, 4, pools, 0)

    s3_1 = scan2(1, s2_1)

    for c in wos:
        c.wait_recv()
    blk = ((ii // 64 == jj // 64).astype(F32) * (1.0 / 64.0)).astype(BF16)

    def finish(o):
        cb, cols = c_s[o], jnp.exp(cols_s[o])
        carried = dot(cb, b_in[o, 0]) * spread(cols, 0) + dot(cb, b_in[o, 1]) * spread(cols, 4)
        g = (y_s[o] + carried) * gate[o]
        ms = dot((g * g).astype(BF16), blk)
        mix_s[...] = (g * lax.rsqrt(ms + EPSILON) * ngain).astype(BF16)

    mine = at(t, 128)
    theirs = at(1 - t, 128)
    swaps = []
    swap_send = one_send(dsend)
    raw_send = one_send(raws)
    out_i = (new(0), new(2))
    far = all_of(xrecv, *out_i)
    sent.append(far)

    def produce(o):
        finish(o)
        for q in range(4):
            cs = slice(q * 256, (q + 1) * 256)
            part = dot(mix_s[theirs, :], woi[q]) + dot(pld_s[o, theirs, :], wop[q])
            dsend[o, :, cs] = part.astype(BF16)
        swaps.append(swap_send(dsend.at[o], drecv.at[o], pair))
        for q in range(4):
            cs = slice(q * 256, (q + 1) * 256)
            own[o, :, cs] = dot(mix_s[mine, :], woi[q]) + dot(pld_s[o, mine, :], wop[q])

    def chip_sum(o):
        swaps[o].wait_recv()
        return (own[o] + drecv[o].astype(F32)).reshape(2, 64, 1024)

    def arrive(hf, s3):
        s3[0].wait()
        s3[1].wait_recv()
        enter(hf)

    def out_half(i, h, value, dev, a=0):
        n = value.shape[0]
        xsend[i, h, a : a + n] = value.astype(BF16)
        rows = pl.ds(a, n)
        start(xsend.at[i, h, rows], xrecv.at[i, h, rows], dev, *out_i)

    arrive(0, s3_0)
    produce(0)
    produce(1)
    raws[...] = chip_sum(0).astype(BF16)
    up, down = [], []
    for q in range(2):
        rows = pl.ds(q * 32, 32)
        up.append(raw_send(raws.at[0, rows], rawr.at[0, rows], to_x))
        down.append(raw_send(raws.at[1, rows], rawr.at[1, rows], to_y))
    chip1 = chip_sum(1)
    out_half(0, 0, chip1[0], to_x)
    own[1, 64:128] = chip1[1]
    arrive(1, s3_1)
    produce(2)
    produce(3)
    chip2 = chip_sum(2)
    out_half(1, 1, chip2[1], to_y)
    for q in range(2):
        a = q * 32
        down[q].wait_recv()
        out_half(0, 1, own[1, 64 + a : 96 + a] + rawr[1, a : a + 32].astype(F32), to_x, a)
        up[q].wait_recv()
        out_half(1, 0, chip2[0, a : a + 32] + rawr[0, a : a + 32].astype(F32), to_y, a)
    own[3] = chip_sum(3).reshape(128, 1024)
    far.wait_recv()
    arrived = (xrecv[0].astype(F32) + xrecv[1].astype(F32)).reshape(128, 1024)
    out[0] = (own[3] + arrived).astype(BF16)
    for c in sent:
        c.wait_send()


N_LOCAL, N_SEND, N_RECV = 27, 26, 74


def body(
    tokens, w_inner, w_gate, w_write, w_read, w_pool_in, w_step, conv_inner, conv_cross, rate_log,
    decay_extra, norm_gain, pool_mix, pool_gain, w_out_inner, w_out_pool,
):
    hbm = pl.BlockSpec(memory_space=pl.ANY)
    V = pltpu.VMEM
    scratch = [
        V((4, 2, T, 512), BF16),
        V((2, 16, 512), BF16),
        V((8, 2, 16, 512), BF16),
        V((8, 8, 16, 512), BF16),
        V((8, 8, 16, 256), BF16),
        V((8, 8, 16, 128), BF16),
        V((16, 512), BF16),
        V((16, 256), BF16),
        V((16, 128), BF16),
        V((4, 256, 256), BF16),
        V((4, 256, 256), BF16),
        V((4, 2, 8, T), F32),
        V((128, 256), BF16),
        V((2, 16, 1024), BF16),
        pltpu.SMEM((2, 32), F32),
        V((5, 256), BF16),
        V((5, 2, 128), BF16),
        V((16, 128), F32),
        V((8, 128), F32),
        V((8, 512), F32),
        V((288, 384), F32),
        V((288, 128), F32),
        V((4, 2, 16, 512), F32),
        V((4, T, 256), F32),
        V((4, T, 256), BF16),
        V((4, T, 128), BF16),
        V((4, T, 128), BF16),
        V((4, 8, T), F32),
        V((4, 8, T), F32),
        V((4, T, 128), F32),
        V((4, T, 256), F32),
        V((2, 4, T, 128), BF16),
        V((T, 3 * T), BF16),
        V((4, 2, 128, 256), F32),
        V((8, 256), F32),
        V((8, 256), F32),
        V((2, 4, 2, 32, 256), BF16),
        V((2, 4, 2, 32, 256), BF16),
        V((4, 8, 256), F32),
        V((4, 8, 256), F32),
        V((2, 8, 2, 32, 256), BF16),
        V((8, 8, 256), F32),
        V((8, 256), F32),
        V((2, 4, 2, 32, 256), F32),
        V((2, 2, 32, 256), BF16),
        V((2, 4, 2, 32, 256), BF16),
        V((4, 2, 128, 256), BF16),
        V((4, 128, 1024), F32),
        V((4, 128, 1024), BF16),
        V((4, 128, 1024), BF16),
        V((2, 64, 1024), BF16),
        V((2, 64, 1024), BF16),
        V((2, 2, 64, 1024), BF16),
        V((2, 2, 64, 1024), BF16),
        V((T, 256), BF16),
        V((4, T, 256), BF16),
        pltpu.SemaphoreType.DMA((N_LOCAL,)),
        pltpu.SemaphoreType.DMA((N_SEND,)),
        pltpu.SemaphoreType.DMA((N_RECV,)),
        pltpu.SemaphoreType.DMA((2, 2)),
    ]
    return pl.pallas_call(
        kernel,
        out_shape=jax.ShapeDtypeStruct((1, 128, 1024), BF16),
        in_specs=[hbm] * 16,
        out_specs=pl.BlockSpec(memory_space=pltpu.VMEM),
        scratch_shapes=scratch,
        compiler_params=pltpu.CompilerParams(
            collective_id=0, has_side_effects=True, vmem_limit_bytes=60 * 1024 * 1024
        ),
    )(
        tokens, w_inner, w_gate, w_write, w_read, w_pool_in, jnp.transpose(w_step, (1, 2, 0)),
        conv_inner, conv_cross, rate_log, jnp.transpose(decay_extra[0], (1, 2, 0)),
        norm_gain.reshape(16, 128), pool_mix, pool_gain.reshape(8, 128), w_out_inner, w_out_pool,
    )


def solution(mesh):
    finer = Mesh(
        mesh.devices.reshape(8, 8, mesh.shape["fs"], mesh.shape["tp"]), ("z", "y", "fs", "tp")
    )
    in_specs = (
        P("fs", SP, "tp"),
        P(SP, "tp"),
        P(SP, "tp"),
        P(SP, "tp"),
        P(SP, "tp"),
        P(SP, "tp"),
        P(),
        P(),
        P(),
        P(),
        P("fs", SP, None, "tp"),
        P(),
        P(),
        P(),
        P("tp", "fs"),
        P("tp", "fs"),
    )
    out_specs = P("fs", ("z", "y", "tp"), None)
    return jax.shard_map(body, mesh=finer, in_specs=in_specs, out_specs=out_specs, check_vma=False)
```

```python
import functools

import jax
import jax.numpy as jnp
from jax import lax
from jax.experimental import pallas as pl
from jax.experimental.pallas import tpu as pltpu
from jax.sharding import Mesh
from jax.sharding import PartitionSpec as P

MESH = pl.DeviceIdType.MESH
F32, BF16 = jnp.float32, jnp.bfloat16
SP = ("z", "y")
EPSILON = 1e-05
T = 256
GRID_W = 32


def silu(v):
    return (0.5 * v) * (1.0 + jnp.tanh(0.5 * v))


def dot(a, b, dims=((1,), (0,)), **kw):
    return lax.dot_general(a, b, (dims, ((), ())), preferred_element_type=F32, **kw)


def kernel(
    tok, w_inner, w_gate, w_write, w_read, w_pool, wst_in, ci_in, cc_in, rate_in, dec_in, ng_in, pmix_in,
    pg_in, woi_in, wop_in,
    out,
    x_b, hrow, hall, wa, wb1, wb2, alt1, alt3, alt4, woi, wop, de, pmix, wst, rate_s, ci, cc, ng, pg, par,
    p_s, p_r, hp, y_s, v_s, b_s, c_s, cum_s, stp_s, cols_s, gate, pool, m_s,
    sb, dec, decp, st, r1, d1, pd, r2, d2, totd, res, tot, inc, b_in, own, dsend, drecv, raws, rawr, xsend, xrecv,
    mix_s, pld_s,
    lsem, ssem, rsem, psem,
):
    z, y, f, t = (lax.axis_index(a) for a in ("z", "y", "fs", "tp"))
    fq, yq, yp = lax.rem(f, 2), lax.rem(y, 2), y // 2
    r = fq * 2 + yq
    sp = z * 8 + y
    group_at = t * 2 + fq

    def along(d):
        v = lax.rem(sp + d, 64)
        return {"z": v // 8, "y": lax.rem(v, 8)}

    count = [0, 0, 0]
    sent = []

    def new(kind):
        count[kind] += 1
        return count[kind] - 1

    def start(src, dst, dev, si, ri):
        c = pltpu.make_async_remote_copy(
            src_ref=src, dst_ref=dst, send_sem=ssem.at[si], recv_sem=rsem.at[ri],
            device_id=dev, device_id_type=MESH,
        )
        c.start()
        return c

    def all_of(ref, si, ri):
        return pltpu.make_async_remote_copy(
            src_ref=ref, dst_ref=ref, send_sem=ssem.at[si], recv_sem=rsem.at[ri],
            device_id={"tp": 1 - t}, device_id_type=MESH,
        )

    def send(src, dst, dev):
        c = start(src, dst, dev, new(0), new(2))
        sent.append(c)
        return c

    def together(items, whole):
        si, ri = new(0), new(2)
        for src, dst, dev in items:
            start(src, dst, dev, si, ri)
        c = all_of(whole, si, ri)
        sent.append(c)
        return c

    def one_send(whole):
        si = new(0)
        sent.append(all_of(whole, si, 0))
        return lambda src, dst, dev: start(src, dst, dev, si, new(2))

    def local(src, dst):
        c = pltpu.make_async_copy(src, dst, lsem.at[count[1]])
        count[1] += 1
        c.start()
        return c

    def ymod(d):
        return lax.rem(y + d, 8)

    def zmod(d):
        return lax.rem(z + d, 8)

    def fmod(d):
        return lax.rem(f + d, 4)

    def pmod(d):
        return lax.rem(yp + d, 4)

    f_flip, y_flip = f + 1 - 2 * fq, y + 1 - 2 * yq
    r_x, r_y, r_d = (1 - fq) * 2 + yq, fq * 2 + 1 - yq, 3 - r
    to_x, to_y, to_d = {"fs": f_flip}, {"y": y_flip}, {"fs": f_flip, "y": y_flip}

    def at(v, n):
        return pl.ds(pl.multiple_of(v * n, n), n)

    near_first = (1, 7, 2, 6, 3, 5, 4)
    pair = {"tp": 1 - t}
    group = [pair] + [{**a, "tp": e} for a in (to_x, to_y, to_d) for e in (t, 1 - t)]
    peers = [{"y": ymod(d)} for d in range(1, 8)] + [{"z": zmod(d)} for d in range(1, 8)]
    peers += group + [{"fs": fmod(d)} for d in range(1, 4)] + [along(d) for d in (1, 63, 2, 62)]

    barrier = pltpu.get_barrier_semaphore()
    for p in peers:
        pl.semaphore_signal(barrier, inc=1, device_id=p, device_id_type=MESH)
    mine1, mine3, mine4 = (w.at[z, y] for w in (wa, wb1, wb2))
    tok_local = local(tok.at[0], x_b.at[r, t])
    w_local = [
        local(w_inner.at[:, at(q, 256)], m.at[:, pl.ds(0, 256)])
        for q, m in ((r, mine1), (r_y, alt1))
    ]
    w_local += [
        local(w.at[:, at(fq, 128)], m.at[:, pl.ds(c, 128)])
        for w, c in ((w_write, 256), (w_read, 384))
        for m in (mine1, alt1)
    ]
    w_local += [
        local(w_gate.at[:, at(r, 256)], mine3),
        local(w_gate.at[:, at(r_y, 256)], alt3),
        local(w_pool.at[:, at(r, 128)], mine4),
        local(w_pool.at[:, at(r_y, 128)], alt4),
    ]
    others = [
        local(wst_in.at[:, at(t, 16)], wst),
        local(dec_in.at[:, at(fq, 8)], de.at[r]),
        local(ci_in.at[:, at(t * 4 + r, 256)], ci),
        local(cc_in.at[:, :, at(group_at, 128)], cc),
        local(ng_in, ng),
        local(rate_in, rate_s),
        local(pg_in, pg),
        local(pmix_in.at[group_at, at(yq, 128)], pmix),
        local(woi_in.at[at(r, 256)], woi.at[f]),
        local(wop_in.at[at(fq, 256)], wop.at[f]),
    ]
    pool[:, 0] = jnp.zeros((2, T, 128), BF16)
    pool[:, 3] = jnp.zeros((2, T, 128), BF16)
    tok_local.wait()
    for c in w_local:
        c.wait()
    pl.semaphore_wait(barrier, len(peers))

    x_own = x_b.at[r, t]
    def stage(w, mine, alt):
        items = [(alt if d % 2 else mine, mine, {"y": ymod(d)}) for d in near_first]
        return together(items, w.at[0, pl.ds(0, 7)])

    first = stage(wa, mine1, alt1)
    edges = together(
        [
            (x_own.at[pl.ds(240, 16)], hrow.at[0], along(1)),
            (x_own.at[pl.ds(0, 16)], hrow.at[1], along(63)),
        ],
        hrow,
    )
    send_x = one_send(x_b.at[pl.ds(0, 2), 0])
    x_right = send_x(x_own, x_own, to_x)
    x_left = send_x(x_own, x_own, to_y)
    pair_i = (new(0), new(2))

    def to_pair(block):
        start(block, block, pair, *pair_i)

    x_pair = all_of(x_b.at[pl.ds(0, 3), 0], *pair_i)
    sent.append(x_pair)
    to_pair(x_own)
    decs = together(
        [
            (dec_in.at[:, at(q, 8)], de.at[r], g)
            for q, g in ((1 - fq, to_x), (fq, to_y), (1 - fq, to_d))
        ],
        de.at[pl.ds(0, 3)],
    )

    rings = {}

    def hop(piece, k, to):
        (w, a, n, only), issue = piece
        if k == 3 and only is None:
            a, n = (a if to == 1 else a + n // 2), n // 2
        s = w.at[zmod(8 - k if to == 1 else k), pl.ds(a, n)]
        return issue(s, s, {"z": zmod(to)})

    def begin(name, w, halves):
        pieces = [(w, i, 2, 1 if i < 4 else 7) for i in range(0, 8, 2)] if halves else [(w, 0, 8, None)]
        issue = one_send(w.at[pl.ds(0, 7)])
        rings[name] = [((p, issue), to, [hop((p, issue), 0, to)]) for p in pieces for to in (1, 7)]

    def step(names, k):
        for name in names:
            for piece, to, ring in rings[name]:
                last = piece[0][3] is not None and piece[0][3] != to
                if k < 4 or not last:
                    ring[k - 1].wait_recv()
                if k < 3 or (k == 3 and not last):
                    ring.append(hop(piece, k, to))

    first.wait_recv()
    begin("a", wa, True)
    edges.wait_recv()
    halo_local = local(hrow, hall.at[r * 2 + t])
    halos = together([(hrow, hall.at[r * 2 + t], g) for g in group], hall.at[pl.ds(0, 7)])
    step(("a",), 1)
    x_right.wait_recv()
    block = x_b.at[r_x, t]
    far_i = (new(0), new(2))
    x_far = all_of(x_b.at[r_d, t], *far_i)
    sent.append(x_far)
    start(block.at[pl.ds(0, 64)], block.at[pl.ds(0, 64)], to_y, *far_i)
    to_pair(block)
    x_left.wait_recv()
    block = x_b.at[r_y, t]
    start(block.at[pl.ds(64, 192)], block.at[pl.ds(64, 192)], to_x, *far_i)
    to_pair(block)
    fourth, third = stage(wb2, mine4, alt4), stage(wb1, mine3, alt3)
    step(("a",), 2)
    for c in others:
        c.wait()
    par[0:5, 0:256] = ci[...].astype(F32)
    par[0:5, 256:384] = cc[:, 0, :].astype(F32)
    par[0:5, 384:512] = cc[:, 1, :].astype(F32)
    ii = lax.broadcasted_iota(jnp.int32, (T, T), 0)
    jj = lax.broadcasted_iota(jnp.int32, (T, T), 1)
    low = lax.broadcasted_iota(jnp.int32, (T, 128), 1) < 64

    def slot_block(o):
        return lax.rem(yq + lax.rem(3 - o, 2), 2)

    def slot_unit(o):
        return lax.rem(fq + (3 - o) // 2, 2) * 2 + slot_block(o)

    r8 = lax.broadcasted_iota(jnp.int32, (8, 1), 0)
    rate = jnp.zeros((8, 1), F32)
    for i in range(8):
        rate = jnp.where(r8 == i, rate_s[i // 4, t * 16 + r * 4 + i % 4], rate)
    rate = jnp.exp(rate)

    def pick(rows, which, n):
        chosen = rows[0:4]
        for i in range(1, n):
            chosen = jnp.where(which == i, rows[4 * i : 4 * i + 4], chosen)
        return chosen

    def decay_rows(o):
        s = slot_unit(o)
        w0, w1 = wst[:, :, 0:512].reshape(32, 512), wst[:, :, 512:1024].reshape(32, 512)
        all_raw = dot(w0, x_b[s, 0], ((1,), (1,))) + dot(w1, x_b[s, 1], ((1,), (1,)))
        raw = jnp.concatenate([pick(all_raw[0:16], r, 4), pick(all_raw[16:32], r, 4)], axis=0)
        extra = jnp.concatenate([pick(de[s, 0], yq, 2), pick(de[s, 1], yq, 2)], axis=0)
        stp = jnp.maximum(raw, 0.0) + jnp.log1p(jnp.exp(-jnp.abs(raw)))
        stp_s[o] = stp
        cum_s[o] = extra - stp * rate

    x_pair.wait_recv()
    decs.wait_recv()
    for o in (3, 2, 1):
        decay_rows(o)
    step(("a",), 3)
    x_far.wait_recv()
    block = x_b.at[r_d, t]
    far_pair = send(block, block, pair)
    fourth.wait_recv()
    begin("b2", wb2, False)
    third.wait_recv()
    begin("b1", wb1, False)
    dests = [(fmod(d), lax.rem(fmod(d), 2)) for d in (1, 3, 2)]
    wos = [
        together(
            [(woi_in.at[at(q * 2 + yq, 256)], woi.at[f], {"fs": g}) for g, q in dests],
            woi.at[pl.ds(0, 3)],
        ),
        together(
            [(wop_in.at[at(q, 256)], wop.at[f], {"fs": g}) for g, q in dests], wop.at[pl.ds(0, 3)]
        ),
    ]
    far_pair.wait_recv()
    decay_rows(0)
    ld = cum_s[...].reshape(32, T)
    ld_a = ld.astype(BF16)
    rest = ld - ld_a.astype(F32)
    ld_b = rest.astype(BF16)
    ld_c = (rest - ld_b.astype(F32)).astype(BF16)
    ld3 = jnp.concatenate([ld_a, ld_b, ld_c], axis=0)
    pre = dot(ld3, (ii <= jj).astype(F32).astype(BF16))
    suf = dot(ld3, (ii >= jj).astype(F32).astype(BF16))
    pre = pre[0:32] + (pre[32:64] + pre[64:96])
    suf = suf[0:32] + (suf[32:64] + suf[64:96])
    fwd_row = lax.rem(lax.broadcasted_iota(jnp.int32, (32, T), 0), 8) < 4
    cum = jnp.where(fwd_row, pre, suf)
    cum_s[...] = cum.reshape(4, 8, T)
    lane4 = lax.broadcasted_iota(jnp.int32, (1, 256), 1) // 64
    ends = []
    for o in range(4):
        for n in range(2):
            row = jnp.zeros((1, 256), F32)
            for h in range(4):
                i = o * 8 + n * 4 + h
                e = cum[i : i + 1, T - 1 : T] if n == 0 else cum[i : i + 1, 0:1]
                row = jnp.where(lane4 == h, e, row)
            ends.append(row)
    dec[...] = jnp.concatenate(ends, axis=0)
    both = [ends[4 * hf + n] + ends[4 * hf + 2 + n] for hf in range(2) for n in range(2)]
    decp[...] = jnp.concatenate(both + [jnp.zeros((4, 256), F32)], axis=0)
    own_dec = local(decp, d1.at[yp])
    sd1 = together([(decp, d1.at[yp], {"y": ymod(2 * d)}) for d in (1, 3, 2)], d1.at[pl.ds(0, 3)])

    halo_local.wait()
    halos.wait_recv()
    step(("a",), 4)
    step(("b2",), 1)

    def rows_of(w, k, n):
        return w[4 * k : 4 * k + 4].reshape(512, n)

    halls = hall[...].reshape(4, 2, 2, 16, 512)
    h0 = halls[:, 0].reshape(128, 512)
    h1 = halls[:, 1].reshape(128, 512)
    hrow_at = lax.broadcasted_iota(jnp.int32, (128, 512), 0)
    side = lax.rem(hrow_at // 16, 2)
    place = sp - yq + lax.rem(hrow_at // 32, 2)
    gone = jnp.logical_or(
        jnp.logical_and(side == 0, place == 0), jnp.logical_and(side == 1, place == 63)
    )
    hproj = (dot(h0, rows_of(wa, 0, 512)) + dot(h1, rows_of(wa, 1, 512))).astype(BF16).astype(F32)
    hp[...] = jnp.where(gone, 0.0, hproj).reshape(4, 2, 16, 512)

    def spread(cols, c):
        parts = [
            jnp.where(low, cols[:, c + 2 * q : c + 2 * q + 1], cols[:, c + 2 * q + 1 : c + 2 * q + 2])
            for q in range(2)
        ]
        return jnp.concatenate(parts, axis=1)

    def convolve(s, x0, x1, buf, c, n):
        cs = slice(c, c + n)
        w0, w1 = (wa[4 * k : 4 * k + 4, :, :, cs].reshape(512, n) for k in range(2))
        buf[16:272, :] = (dot(x0, w0) + dot(x1, w1)).astype(BF16).astype(F32)
        buf[0:16, :] = hp[s, 0, :, cs]
        buf[272:288, :] = hp[s, 1, :, cs]
        conv = buf[14 : 14 + T, :] * par[0:1, cs]
        for j in range(1, 5):
            conv = conv + buf[14 + j : 14 + j + T, :] * par[j : j + 1, cs]
        return silu(conv)

    def front(o):
        s = slot_unit(o)
        x0, x1 = x_b[s, 0], x_b[s, 1]
        act = convolve(s, x0, x1, p_s, 0, 384)
        v, b = act[:, 0:256], act[:, 256:384]
        cols = jnp.concatenate([cum_s[o], stp_s[o], jnp.zeros((112, T), F32)], axis=0).T
        cols_s[o] = cols
        v_s[o] = v.astype(BF16)
        b_s[o] = b.astype(BF16)
        bt = b.T.astype(BF16)
        lane = lax.broadcasted_iota(jnp.int32, (1, 128), 1)
        end = jnp.where(lane < 4, cols[T - 1 : T, :], cols[0:1, :])
        w_end = jnp.exp(end - cols)
        for n in range(2):
            scale = spread(w_end, 4 * n) * spread(cols, 8 + 4 * n)
            sb[o, n] = dot(bt, (v * scale).astype(BF16))

    def early_late(hf):
        return 2 * hf + 1 - yq, 2 * hf + yq

    def fade(o, n):
        return jnp.exp(dec[pl.ds(2 * o + n, 1), :])

    def join(hf):
        e, l = early_late(hf)
        ahead = sb[e, 0] * fade(l, 0) + sb[l, 0]
        behind = sb[l, 1] * fade(e, 1) + sb[e, 1]
        st[hf, :, 0] = ahead.astype(BF16).reshape(4, 32, 256)
        st[hf, :, 1] = behind.astype(BF16).reshape(4, 32, 256)

    def enter(hf):
        e, l = early_late(hf)
        ahead = inc[hf, :, 0].reshape(128, 256)
        behind = inc[hf, :, 1].reshape(128, 256)
        b_in[e, 0] = ahead
        b_in[l, 0] = (ahead.astype(F32) * fade(e, 0) + sb[e, 0]).astype(BF16)
        b_in[l, 1] = behind
        b_in[e, 1] = (behind.astype(F32) * fade(l, 1) + sb[l, 1]).astype(BF16)

    s1, own_st = [], []
    for hf in range(2):

        def front_step(o, _):
            front(o)
            return _

        lax.fori_loop(2 * hf, 2 * hf + 2, front_step, 0)
        join(hf)
        own_st.append(local(st.at[hf, yp], r1.at[hf, yp]))
        items = [(st.at[hf, pmod(d)], r1.at[hf, yp], {"y": ymod(2 * d)}) for d in (1, 3, 2)]
        s1.append(together(items, r1.at[hf, pl.ds(0, 3)]))
        step(("b2",), hf + 2)
        step(("b1",), hf + 1)
        if hf == 0:
            own_dec.wait()
            sd1.wait_recv()
            cumf = jnp.zeros((8, 256), F32)
            cumb = jnp.zeros((8, 256), F32)
            back = lax.rem(lax.broadcasted_iota(jnp.int32, (8, 256), 0), 2) == 1
            pf = []
            for i in range(4):
                pf.append(cumf)
                cumf = cumf + d1[i]
            for i in reversed(range(4)):
                pd[i] = jnp.exp(jnp.where(back, cumb, pf[i]))
                cumb = cumb + d1[i]
            totd[...] = cumf
            items = [(totd, d2.at[z], {"z": zmod(d)}) for d in near_first]
            sd2 = together(items, d2.at[pl.ds(0, 7)])

    def inner(o, _):
        s = slot_unit(o)
        c_s[o] = convolve(s, x_b[s, 0], x_b[s, 1], p_r, 384, 128).astype(BF16)
        cols, cu, stp = cols_s[o], cum_s[o], stp_s[o]
        scores = dot(c_s[o], b_s[o], ((1,), (1,)))
        for q in range(2):
            vp = v_s[o, :, q * 128 : (q + 1) * 128]
            both = []
            for e in range(2):
                h = 2 * q + e
                expo = jnp.where(
                    jj <= ii,
                    cols[:, h : h + 1] - cu[h : h + 1, :],
                    cols[:, 4 + h : 5 + h] - cu[4 + h : 5 + h, :],
                )
                df, db = stp[h : h + 1, :], stp[4 + h : 5 + h, :]
                dts = jnp.where(jj < ii, df, jnp.where(jj > ii, db, df + db))
                both.append(dot((scores * jnp.exp(expo) * dts).astype(BF16), vp))
            y_s[o, :, q * 128 : (q + 1) * 128] = jnp.where(low, both[0], both[1])
        return _

    def scan1(hf):
        own_st[hf].wait()
        s1[hf].wait_recv()
        for n in range(2):
            run = jnp.zeros((32, 256), F32)
            for i in range(4) if n == 0 else reversed(range(4)):
                res[hf, i, n] = run
                w = jnp.exp(d1[i, 2 * hf + n : 2 * hf + n + 1, :])
                run = run * w + r1[hf, i, n].astype(F32)
            tot[hf, n] = run.astype(BF16)
        items = [
            (tot.at[hf, (z + d) // 8], r2.at[hf, z, (z + d) // 8], {"z": zmod(d)})
            for d in near_first
        ]
        return together(items, r2.at[hf, pl.ds(0, 7), 0])

    def scan2(hf, s2):
        s2.wait_recv()
        for n in range(2):
            acc = jnp.zeros((32, 256), F32)
            for i in range(8) if n == 0 else reversed(range(8)):
                w = jnp.exp(d2[i, 2 * hf + n : 2 * hf + n + 1, :])
                new = acc * w + r2[hf, i, n].astype(F32)
                used = (i < z) if n == 0 else (i > z)
                acc = jnp.where(used, new, acc)
            for i in range(4):
                w = pd[i, 2 * hf + n : 2 * hf + n + 1, :]
                r1[hf, i, n] = (res[hf, i, n] + acc * w).astype(BF16)
        mine = local(r1.at[hf, yp], inc.at[hf, yp])
        items = [(r1.at[hf, pmod(d)], inc.at[hf, yp], {"y": ymod(2 * d)}) for d in (1, 3, 2)]
        return mine, together(items, inc.at[hf, pl.ds(0, 3)])

    def gates(o, _):
        s = slot_unit(o)
        g = dot(x_b[s, 0], rows_of(wb1, 0, 256)) + dot(x_b[s, 1], rows_of(wb1, 1, 256))
        gate[o] = silu(g.astype(BF16).astype(F32))
        return _

    def grids(o, _):
        s = slot_unit(o)
        q = dot(x_b[s, 0], rows_of(wb2, 0, 128)) + dot(x_b[s, 1], rows_of(wb2, 1, 128))
        pool[o // 2, 1 + slot_block(o)] = q.astype(BF16)
        return _

    def pool_copies(g):
        n = GRID_W << g
        spans = ((2, 0, T - n, along(2)), (1, 3, 0, along(62)))
        return [
            pltpu.make_async_remote_copy(
                src_ref=pool.at[:, a, pl.ds(c, n)], dst_ref=pool.at[:, b, pl.ds(c, n)],
                send_sem=psem.at[0, i], recv_sem=psem.at[1, i], device_id=dev, device_id_type=MESH,
            )
            for i, (a, b, c, dev) in enumerate(spans)
        ]

    lax.fori_loop(0, 2, inner, 0)
    k = jnp.left_shift(jnp.int32(2), group_at)
    ti = lax.broadcasted_iota(jnp.int32, (T, 3 * T), 0)
    tj = lax.broadcasted_iota(jnp.int32, (T, 3 * T), 1)
    ri, ci_ = ti // GRID_W + 8, lax.rem(ti, GRID_W)
    rj, cj = tj // GRID_W, lax.rem(tj, GRID_W)
    inside = (rj >= ri - k // 2) & (rj < ri + k // 2) & (cj >= ci_ - k // 2) & (cj < ci_ + k // 2)
    m_s[...] = inside.astype(F32).astype(BF16)
    s2_0 = scan1(0)
    step(("b2",), 4)
    lax.fori_loop(0, 4, grids, 0)
    for g in range(4):

        @pl.when(group_at == g)
        def _():
            for c in pool_copies(g):
                c.start()

    step(("b1",), 3)
    s2_1 = scan1(1)
    lax.fori_loop(2, 4, inner, 0)
    sd2.wait_recv()
    s3_0 = scan2(0, s2_0)
    step(("b1",), 4)
    lax.fori_loop(0, 4, gates, 0)
    for g in range(4):

        @pl.when(group_at == g)
        def _():
            for c in pool_copies(g):
                c.wait()
    pool[:, 0] = jnp.where(sp // 2 == 0, jnp.zeros((2, T, 128), BF16), pool[:, 0])
    pool[:, 3] = jnp.where(sp // 2 == 31, jnp.zeros((2, T, 128), BF16), pool[:, 3])
    col = lax.rem(lax.broadcasted_iota(jnp.int32, (T, 128), 0), GRID_W)
    cols_in = jnp.minimum(col + k // 2, GRID_W) - jnp.maximum(col - k // 2, 0)
    pgain = jnp.concatenate([pg[pl.ds(2 * group_at + i, 1), :] for i in range(2)], axis=1)
    ngain = jnp.concatenate([ng[pl.ds(8 * t + 2 * r + i, 1), :] for i in range(2)], axis=1)

    def pools(o, _):
        b = slot_block(o)
        row = lax.broadcasted_iota(jnp.int32, (T, 128), 0) // GRID_W + (sp - yq + b) * 8
        cells = (jnp.minimum(row + k // 2, 512) - jnp.maximum(row - k // 2, 0)) * cols_in
        rows = jnp.concatenate([pool[o // 2, b + i] for i in range(3)], axis=0)
        off = dot(m_s[...], rows) / cells.astype(F32) - pool[o // 2, b + 1].astype(F32)
        pld_s[o] = (dot(off.astype(BF16), pmix[...]) * pgain).astype(BF16)
        return _

    lax.fori_loop(0, 4, pools, 0)

    s3_1 = scan2(1, s2_1)

    for c in wos:
        c.wait_recv()
    blk = ((ii // 64 == jj // 64).astype(F32) * (1.0 / 64.0)).astype(BF16)

    def finish(o):
        cb, cols = c_s[o], jnp.exp(cols_s[o])
        carried = dot(cb, b_in[o, 0]) * spread(cols, 0) + dot(cb, b_in[o, 1]) * spread(cols, 4)
        g = (y_s[o] + carried) * gate[o]
        ms = dot((g * g).astype(BF16), blk)
        mix_s[...] = (g * lax.rsqrt(ms + EPSILON) * ngain).astype(BF16)

    mine = at(t, 128)
    theirs = at(1 - t, 128)
    swaps = []
    swap_send = one_send(dsend)
    raw_send = one_send(raws)
    out_i = (new(0), new(2))
    far = all_of(xrecv, *out_i)
    sent.append(far)

    def produce(o):
        finish(o)
        for q in range(4):
            cs = slice(q * 256, (q + 1) * 256)
            part = dot(mix_s[theirs, :], woi[q]) + dot(pld_s[o, theirs, :], wop[q])
            dsend[o, :, cs] = part.astype(BF16)
        swaps.append(swap_send(dsend.at[o], drecv.at[o], pair))
        for q in range(4):
            cs = slice(q * 256, (q + 1) * 256)
            own[o, :, cs] = dot(mix_s[mine, :], woi[q]) + dot(pld_s[o, mine, :], wop[q])

    def chip_sum(o):
        swaps[o].wait_recv()
        return (own[o] + drecv[o].astype(F32)).reshape(2, 64, 1024)

    def arrive(hf, s3):
        s3[0].wait()
        s3[1].wait_recv()
        enter(hf)

    def out_half(i, h, value, dev, a=0):
        n = value.shape[0]
        xsend[i, h, a : a + n] = value.astype(BF16)
        rows = pl.ds(a, n)
        start(xsend.at[i, h, rows], xrecv.at[i, h, rows], dev, *out_i)

    arrive(0, s3_0)
    produce(0)
    produce(1)
    raws[...] = chip_sum(0).astype(BF16)
    up, down = [], []
    for q in range(2):
        rows = pl.ds(q * 32, 32)
        up.append(raw_send(raws.at[0, rows], rawr.at[0, rows], to_x))
        down.append(raw_send(raws.at[1, rows], rawr.at[1, rows], to_y))
    arrive(1, s3_1)
    produce(2)
    chip1 = chip_sum(1)
    out_half(0, 0, chip1[0], to_x)
    own[1, 64:128] = chip1[1]
    produce(3)
    chip2 = chip_sum(2)
    out_half(1, 1, chip2[1], to_y)
    for q in range(2):
        a = q * 32
        down[q].wait_recv()
        out_half(0, 1, own[1, 64 + a : 96 + a] + rawr[1, a : a + 32].astype(F32), to_x, a)
        up[q].wait_recv()
        out_half(1, 0, chip2[0, a : a + 32] + rawr[0, a : a + 32].astype(F32), to_y, a)
    own[3] = chip_sum(3).reshape(128, 1024)
    far.wait_recv()
    arrived = (xrecv[0].astype(F32) + xrecv[1].astype(F32)).reshape(128, 1024)
    out[0] = (own[3] + arrived).astype(BF16)
    for c in sent:
        c.wait_send()


N_LOCAL, N_SEND, N_RECV = 27, 26, 74


def body(
    tokens, w_inner, w_gate, w_write, w_read, w_pool_in, w_step, conv_inner, conv_cross, rate_log,
    decay_extra, norm_gain, pool_mix, pool_gain, w_out_inner, w_out_pool,
):
    hbm = pl.BlockSpec(memory_space=pl.ANY)
    V = pltpu.VMEM
    scratch = [
        V((4, 2, T, 512), BF16),
        V((2, 16, 512), BF16),
        V((8, 2, 16, 512), BF16),
        V((8, 8, 16, 512), BF16),
        V((8, 8, 16, 256), BF16),
        V((8, 8, 16, 128), BF16),
        V((16, 512), BF16),
        V((16, 256), BF16),
        V((16, 128), BF16),
        V((4, 256, 256), BF16),
        V((4, 256, 256), BF16),
        V((4, 2, 8, T), F32),
        V((128, 256), BF16),
        V((2, 16, 1024), BF16),
        pltpu.SMEM((2, 32), F32),
        V((5, 256), BF16),
        V((5, 2, 128), BF16),
        V((16, 128), F32),
        V((8, 128), F32),
        V((8, 512), F32),
        V((288, 384), F32),
        V((288, 128), F32),
        V((4, 2, 16, 512), F32),
        V((4, T, 256), F32),
        V((4, T, 256), BF16),
        V((4, T, 128), BF16),
        V((4, T, 128), BF16),
        V((4, 8, T), F32),
        V((4, 8, T), F32),
        V((4, T, 128), F32),
        V((4, T, 256), F32),
        V((2, 4, T, 128), BF16),
        V((T, 3 * T), BF16),
        V((4, 2, 128, 256), F32),
        V((8, 256), F32),
        V((8, 256), F32),
        V((2, 4, 2, 32, 256), BF16),
        V((2, 4, 2, 32, 256), BF16),
        V((4, 8, 256), F32),
        V((4, 8, 256), F32),
        V((2, 8, 2, 32, 256), BF16),
        V((8, 8, 256), F32),
        V((8, 256), F32),
        V((2, 4, 2, 32, 256), F32),
        V((2, 2, 32, 256), BF16),
        V((2, 4, 2, 32, 256), BF16),
        V((4, 2, 128, 256), BF16),
        V((4, 128, 1024), F32),
        V((4, 128, 1024), BF16),
        V((4, 128, 1024), BF16),
        V((2, 64, 1024), BF16),
        V((2, 64, 1024), BF16),
        V((2, 2, 64, 1024), BF16),
        V((2, 2, 64, 1024), BF16),
        V((T, 256), BF16),
        V((4, T, 256), BF16),
        pltpu.SemaphoreType.DMA((N_LOCAL,)),
        pltpu.SemaphoreType.DMA((N_SEND,)),
        pltpu.SemaphoreType.DMA((N_RECV,)),
        pltpu.SemaphoreType.DMA((2, 2)),
    ]
    return pl.pallas_call(
        kernel,
        out_shape=jax.ShapeDtypeStruct((1, 128, 1024), BF16),
        in_specs=[hbm] * 16,
        out_specs=pl.BlockSpec(memory_space=pltpu.VMEM),
        scratch_shapes=scratch,
        compiler_params=pltpu.CompilerParams(
            collective_id=0, has_side_effects=True, vmem_limit_bytes=60 * 1024 * 1024
        ),
    )(
        tokens, w_inner, w_gate, w_write, w_read, w_pool_in, jnp.transpose(w_step, (1, 2, 0)),
        conv_inner, conv_cross, rate_log, jnp.transpose(decay_extra[0], (1, 2, 0)),
        norm_gain.reshape(16, 128), pool_mix, pool_gain.reshape(8, 128), w_out_inner, w_out_pool,
    )


def solution(mesh):
    finer = Mesh(
        mesh.devices.reshape(8, 8, mesh.shape["fs"], mesh.shape["tp"]), ("z", "y", "fs", "tp")
    )
    in_specs = (
        P("fs", SP, "tp"),
        P(SP, "tp"),
        P(SP, "tp"),
        P(SP, "tp"),
        P(SP, "tp"),
        P(SP, "tp"),
        P(),
        P(),
        P(),
        P(),
        P("fs", SP, None, "tp"),
        P(),
        P(),
        P(),
        P("tp", "fs"),
        P("tp", "fs"),
    )
    out_specs = P("fs", ("z", "y", "tp"), None)
    return jax.shard_map(body, mesh=finer, in_specs=in_specs, out_specs=out_specs, check_vma=False)
```
